128 devices in a mesh: sp: 32 (over z, y, core), tp: 4 (over x).
Axes of the slice: x: 4, y: 4, z: 4, core: 2. Of those that a mesh axis runs over, the one named last changes fastest.
Arguments:
- layer_input: bfloat16 [24576, 2048], P('sp', 'tp'), may hold values from -6 to 6
- input_norm_gain: bfloat16 [2048], replicated, may hold values from 0.099609375 to 1.8984375
- query_weight: bfloat16 [2048, 2048], P(None, 'tp'), may hold values from -0.125 to 0.125
- forget_weight: bfloat16 [2048, 2048], P(None, 'tp'), may hold values from -0.125 to 0.125
- value_matrix: bfloat16 [2048, 2048], P(None, 'tp'), may hold values from -0.125 to 0.125
- output_gate_weight: bfloat16 [2048, 2048], P(None, 'tp'), may hold values from -0.125 to 0.125
- after_gate_weight: bfloat16 [2048, 2048], P(None, 'tp'), may hold values from -0.125 to 0.125
- before_gate_weight: bfloat16 [2048, 2048], P(None, 'tp'), may hold values from -0.125 to 0.125
- convolution_input_weight: bfloat16 [2048, 2048], P(None, 'tp'), may hold values from -0.125 to 0.125
- forget_minimum: float32 [2048], P('tp'), may hold values from 0.95 to 0.99999593
- surge_log_decay: float32 [24576, 2048], P('sp', 'tp'), may hold values from -2.2 to 0
- convolution_kernel: bfloat16 [3, 2048], P(None, 'tp'), may hold values from -4 to 4
- head_norm_gain: bfloat16 [128], replicated, may hold values from 0.099609375 to 1.8984375
- starting_state: float32 [16, 128, 128], P('tp', 'sp'), may hold values from -0.046875 to 0.046875
- recurrence_output_weight: bfloat16 [2048, 2048], P('tp'), may hold values from -0.09375 to 0.09375
- convolution_output_weight: bfloat16 [2048, 2048], P('tp'), may hold values from -0.09375 to 0.09375
- output_norm_gain: bfloat16 [2048], replicated, may hold values from 0.099609375 to 1.8984375
Outputs:
- layer_out: bfloat16 [24576, 2048], P(('sp', 'tp'))
The draws below stay inside these ranges and needn't reach their ends.
All inputs are finite; a program needn't handle non-finite values.
Results may differ from the reference program's by a relative error of at most 0.014.
Values may be sent and summed in bfloat16 or wider, within the bound.
A program may use at most 128 MiB of HBM per device.

```python
import jax
import jax.numpy as jnp
from jax import lax

D = 2048
HEADS = 16
DK = 128
DV = 128
CW = 2048
CK = 3
BLK = 64
TOKENS_PER_SHARD = 768
TOKENS = 24576
KEYW = 2048
VALW = 2048


def decay_tables(key):
    keys = jax.random.split(jax.random.fold_in(key, 11), 6)
    share = 0.5
    slow_head = jax.random.uniform(keys[0], (HEADS,), jnp.float32) < share
    slow = jnp.repeat(slow_head, DK)
    rate = jnp.exp(jax.random.uniform(keys[1], (HEADS * DK,), jnp.float32, jnp.log(0.1), jnp.log(0.6))) / TOKENS
    fast_floor = jax.random.uniform(keys[2], (HEADS * DK,), jnp.float32, 0.95, 0.99)
    forget_minimum = jnp.where(slow, 1.0 - rate, fast_floor)
    extra_decay = jnp.where(slow, rate, 0.03)
    decay_factor = jnp.exp(jax.random.uniform(keys[3], (TOKENS // TOKENS_PER_SHARD,), jnp.float32, jnp.log(0.5), jnp.log(2.0)))
    spots = jax.random.randint(keys[4], (3,), 0, TOKENS)
    losses = jnp.log(jax.random.uniform(keys[5], (3,), jnp.float32, 0.5, 0.8))
    position = jnp.arange(TOKENS)
    decay_surge = jnp.sum(jnp.where(position[:, None] == spots[None, :], losses[None, :], 0.0), axis=1)
    surge_log_decay = -jnp.repeat(decay_factor, TOKENS_PER_SHARD)[:, None] * extra_decay[None, :] + decay_surge[:, None]
    return (forget_minimum.astype(jnp.float32), surge_log_decay.astype(jnp.float32))


def draw_forget_minimum(key, part):
    return decay_tables(key)[0]


def draw_surge_log_decay(key, part):
    return decay_tables(key)[1]


def shard_levels(key, shape, pieces, least, largest):
    factor_of, own = 1.0, jax.random.fold_in(key, 6)
    for dim, blocks in pieces:
        draws = jnp.exp(jax.random.uniform(jax.random.fold_in(own, dim), (blocks,), jnp.float32, least / len(pieces), largest / len(pieces)))
        factor_of = factor_of * jnp.repeat(draws, shape[dim] // blocks).reshape([-1 if axis == dim else 1 for axis in range(len(shape))])
    return factor_of


def normal_values(key, dims, deviation, limit, cuts=(), held_as=jnp.bfloat16):
    entries = jax.random.normal(key, dims, jnp.float32) * deviation
    if len(cuts) > 0:
        entries = shard_levels(key, dims, cuts, -0.22, 0.18) * entries
    return jnp.clip(entries, min=-limit, max=limit).astype(held_as)


def setup_inputs(seed: int = 0) -> dict:
    key_list = jax.random.split(jax.random.key(seed), 18)
    return {
        "layer_input": normal_values(key_list[0], (TOKENS, D), 1.0, 6.0, ((0, 32), (1, 4))),
        "input_norm_gain": jnp.clip(1.0 + 0.18 * jax.random.normal(key_list[1], (D,), jnp.float32), 0.099609375, 1.8984375).astype(jnp.bfloat16),
        "query_weight": normal_values(key_list[2], (D, KEYW), D ** -0.5, 0.125, ((1, 4),)),
        "forget_weight": normal_values(key_list[3], (D, KEYW), D ** -0.5, 0.125, ((1, 4),)),
        "value_matrix": normal_values(key_list[4], (D, VALW), D ** -0.5, 0.125, ((1, 4),)),
        "output_gate_weight": normal_values(key_list[5], (D, VALW), D ** -0.5, 0.125, ((1, 4),)),
        "after_gate_weight": normal_values(key_list[6], (D, CW), D ** -0.5, 0.125, ((1, 4),)),
        "before_gate_weight": normal_values(key_list[7], (D, CW), D ** -0.5, 0.125, ((1, 4),)),
        "convolution_input_weight": normal_values(key_list[8], (D, CW), D ** -0.5, 0.125, ((1, 4),)),
        "forget_minimum": draw_forget_minimum(jax.random.fold_in(key_list[17], 71), 0),
        "surge_log_decay": draw_surge_log_decay(jax.random.fold_in(key_list[17], 71), 0),
        "convolution_kernel": normal_values(key_list[11], (CK, CW), 0.577, 4.0, ((1, 4),)),
        "head_norm_gain": jnp.clip(1.0 + 0.18 * jax.random.normal(key_list[12], (DV,), jnp.float32), 0.099609375, 1.8984375).astype(jnp.bfloat16),
        "starting_state": normal_values(key_list[13], (HEADS, DK, DV), (0.5 * TOKENS ** -0.5), 0.046875, ((0, 4), (1, 32)), jnp.float32),
        "recurrence_output_weight": normal_values(key_list[14], (VALW, D), (VALW + CW) ** -0.5, 0.09375, ((0, 4),)),
        "convolution_output_weight": normal_values(key_list[15], (CW, D), (VALW + CW) ** -0.5, 0.09375, ((0, 4),)),
        "output_norm_gain": jnp.clip(1.0 + 0.18 * jax.random.normal(key_list[16], (D,), jnp.float32), 0.099609375, 1.8984375).astype(jnp.bfloat16),
    }


EPS = 1e-06
PRECISE_PRODUCT = lax.Precision.HIGHEST

def rms_scale(value_rows):
    return lax.rsqrt(lax.optimization_barrier(jnp.mean(value_rows * value_rows, axis=-1, keepdims=True)) + EPS)

def project(normed, weight):
    return jnp.dot(normed, weight, preferred_element_type=jnp.float32).astype(jnp.bfloat16)

def block_pass(latent_state, inputs):
    query_rows, key_inputs, value_rows, forget_gate_logits = inputs
    cumulative_decay = jnp.cumsum(forget_gate_logits, axis=1)
    length = query_rows.shape[1]
    causal_masking = jnp.tril(jnp.ones((length, length), dtype=bool))[None, :, :, None]
    crossed_output = jnp.einsum('rmq,rqu->rmu', query_rows * jnp.exp(cumulative_decay), latent_state, precision=PRECISE_PRODUCT)
    decay = jnp.exp(jnp.where(causal_masking, cumulative_decay[:, :, None, :] - cumulative_decay[:, None, :, :], -jnp.inf))
    scores = jnp.einsum('htk,hsk,htsk->hts', query_rows, key_inputs, decay, precision=PRECISE_PRODUCT)
    o_intra = jnp.einsum('hts,hsv->htv', scores, value_rows, precision=PRECISE_PRODUCT)
    final_state = cumulative_decay[:, -1:, :]
    latent_state = jnp.exp(final_state[:, 0, :])[..., None] * latent_state + jnp.einsum('xar,xai->xri', key_inputs * jnp.exp(final_state - cumulative_decay), value_rows, precision=PRECISE_PRODUCT)
    return (latent_state, o_intra + crossed_output)

def reference(layer_input, input_norm_gain, query_weight, forget_weight, value_matrix, output_gate_weight, after_gate_weight, before_gate_weight, convolution_input_weight, forget_minimum, surge_log_decay, convolution_kernel, head_norm_gain, starting_state, recurrence_output_weight, convolution_output_weight, output_norm_gain):
    rows_f = layer_input.astype(jnp.float32)
    normed = (rows_f * rms_scale(rows_f) * input_norm_gain.astype(jnp.float32)).astype(jnp.bfloat16)
    query_raw = project(normed, query_weight)
    forget_raw = project(normed, forget_weight)
    value_raw = project(normed, value_matrix)
    outgate_raw = project(normed, output_gate_weight)
    postgate_raw = project(normed, after_gate_weight)
    pregate_raw = project(normed, before_gate_weight)
    convval_raw = project(normed, convolution_input_weight)
    forget_single = forget_raw.astype(jnp.float32)
    forget_gate_logits = jnp.logaddexp(jnp.log(forget_minimum), jnp.log1p(-forget_minimum) + jax.nn.log_sigmoid(forget_single)) + surge_log_decay
    key_inputs = (1.0 - forget_minimum) * jax.nn.sigmoid(-forget_single)
    query_rows = jax.nn.silu(query_raw.astype(jnp.float32)) * DK ** (-0.5)
    blocks = TOKENS // BLK

    def to_blocks(value_rows, width):
        return value_rows.reshape(blocks, BLK, HEADS, width).transpose(0, 2, 1, 3)
    _, outputs = lax.scan(block_pass, starting_state.astype(jnp.float32), (to_blocks(query_rows, DK), to_blocks(key_inputs, DK), to_blocks(value_raw.astype(jnp.float32), DV), to_blocks(forget_gate_logits, DK)))
    recurrence_step = outputs.transpose(0, 2, 1, 3).reshape(TOKENS, HEADS, DV)
    normed_heads = recurrence_step * rms_scale(recurrence_step) * head_norm_gain.astype(jnp.float32)
    rec_out = (normed_heads.reshape(TOKENS, HEADS * DV) * jax.nn.silu(outgate_raw.astype(jnp.float32))).astype(jnp.bfloat16)
    mixed_in = pregate_raw.astype(jnp.float32) * convval_raw.astype(jnp.float32)
    padded = jnp.concatenate([jnp.zeros((CK - 1, mixed_in.shape[1]), jnp.float32), mixed_in], axis=0)
    taps_f = convolution_kernel.astype(jnp.float32)
    conv_sum = padded[0:TOKENS] * taps_f[0]
    for offset in range(1, CK):
        conv_sum = conv_sum + padded[offset:offset + TOKENS] * taps_f[offset]
    conv_out = (postgate_raw.astype(jnp.float32) * conv_sum).astype(jnp.bfloat16)
    mixed = jnp.dot(rec_out, recurrence_output_weight, preferred_element_type=jnp.float32) + jnp.dot(conv_out, convolution_output_weight, preferred_element_type=jnp.float32)
    return (mixed * rms_scale(mixed) * output_norm_gain.astype(jnp.float32)).astype(jnp.bfloat16)
```

```python
import jax
import jax.numpy as jnp
from jax import lax
from jax.experimental import pallas as pl
from jax.experimental.pallas import tpu as pltpu
from jax.sharding import PartitionSpec as P

DK = 128
DV = 128
BLK = 64
EPS = 1e-06
MESH = pl.DeviceIdType.MESH
F32 = jnp.float32
BF16 = jnp.bfloat16
VMEM_LIMIT = 62 * 1024 * 1024

NT = (((1,), (1,)), ((), ()))
TN = (((0,), (0,)), ((), ()))


def dot(a, b, dims=None):
    if dims is None:
        return jnp.dot(a, b, preferred_element_type=F32)
    return lax.dot_general(a, b, dims, preferred_element_type=F32)


def sigmoid(v):
    return 1.0 / (1.0 + jnp.exp(-v))


def log_one_minus(u):
    return -u * (1.0 + u * (1 / 2 + u * (1 / 3 + u * (1 / 4 + u * (1 / 5 + u * (1 / 6))))))


def greet(axis, peers):
    barrier = pltpu.get_barrier_semaphore()
    for peer in peers:
        pl.semaphore_signal(barrier, inc=1, device_id={axis: peer}, device_id_type=MESH)
    pl.semaphore_wait(barrier, len(peers))


def gather_project(chunks, n_sp, *refs):
    x, gain, surge, fmin, taps = refs[:5]
    ws = refs[5:12]
    part, qs, og, cv, hd, rim, st = refs[12:19]
    (xl, xr, xo, xn, wv, sv, pr, mx, state, run, tri2, wsem, ssem) = refs[19:32]
    s_or, s_ol, s_fr, s_fl, r_l, r_r, r_oa, r_ob = refs[32:40]
    tokens, width = x.shape
    tc = tokens // chunks
    half = tc // 2
    heads = width // DK
    own_rows = DK // n_sp
    me = lax.axis_index("tp")
    right, left, opp = lax.rem(me + 1, 4), lax.rem(me + 3, 4), lax.rem(me + 2, 4)
    srcs = (me, left, right, opp)

    loads = []
    for k in range(len(ws)):
        for r in range(4):
            rows = pl.ds(pl.multiple_of(srcs[r] * width, width), width)
            loads.append(
                pltpu.make_async_copy(
                    ws[k].at[rows, :], wv.at[k, pl.ds(r * width, width), :], wsem.at[k, r]
                )
            )
    for copy in loads:
        copy.start()
    surge_load = pltpu.make_async_copy(surge, sv, ssem)
    surge_load.start()

    greet("tp", (left, right))

    def rows_of(c, size, off=0):
        return pl.ds(pl.multiple_of(c * tc + off, 16), size)

    def own(c, to_right):
        rows = rows_of(c, tc)
        return pltpu.make_async_remote_copy(
            src_ref=x.at[rows, :],
            dst_ref=(xl if to_right else xr).at[rows, :],
            send_sem=(s_or if to_right else s_ol).at[c],
            recv_sem=(r_l if to_right else r_r).at[c],
            device_id={"tp": right if to_right else left},
            device_id_type=MESH,
        )

    def forward(c, to_right):
        rows = rows_of(c, half, 0 if to_right else half)
        return pltpu.make_async_remote_copy(
            src_ref=(xl if to_right else xr).at[rows, :],
            dst_ref=xo.at[rows, :],
            send_sem=(s_fr if to_right else s_fl).at[c],
            recv_sem=(r_oa if to_right else r_ob).at[c],
            device_id={"tp": right if to_right else left},
            device_id_type=MESH,
        )

    def pass_on(c):
        own(c, True).wait_recv()
        forward(c, True).start()
        own(c, False).wait_recv()
        forward(c, False).start()

    lead = min(2, chunks)
    for c in range(lead):
        own(c, True).start()
        own(c, False).start()

    state[...] = jnp.zeros_like(state)
    run[...] = jnp.zeros_like(run)
    mx[...] = jnp.zeros_like(mx)
    row = lax.broadcasted_iota(jnp.int32, (BLK, 2 * BLK), 0)
    col = lax.broadcasted_iota(jnp.int32, (BLK, 2 * BLK), 1)
    tri2[...] = jnp.where(row >= lax.rem(col, BLK), 1.0, 0.0).astype(BF16)

    pass_on(0)
    if chunks > lead:
        own(lead, True).start()
        own(lead, False).start()
    for copy in loads:
        copy.wait()
    surge_load.wait()

    def chunk(c, carry):
        @pl.when(c + 1 < chunks)
        def _():
            pass_on(c + 1)

        @pl.when(c + 1 + lead < chunks)
        def _():
            own(c + 1 + lead, True).start()
            own(c + 1 + lead, False).start()

        forward(c, True).wait_recv()
        forward(c, False).wait_recv()

        rows = rows_of(c, tc)
        total = jnp.zeros((tc, 1), F32)
        for piece in (x, xl, xr, xo):
            v = piece[rows, :].astype(F32)
            total = total + jnp.sum(v * v, axis=1, keepdims=True)
        scale = lax.rsqrt(total * (1.0 / (4 * width)) + EPS)
        for r, piece in enumerate((x, xl, xr, xo)):
            g = gain[srcs[r]].astype(F32)
            v = piece[rows, :].astype(F32) * scale * g
            xn[:, r * width : (r + 1) * width] = v.astype(BF16)

        def project(k, carry):
            pr[k] = dot(xn[...], wv[k]).astype(BF16)
            return carry

        lax.fori_loop(0, len(ws), project, 0)

        for b in range(tc // BLK):
            lr = slice(b * BLK, (b + 1) * BLK)
            gr = rows_of(c, BLK, b * BLK)
            for h in range(heads):
                ln = slice(h * DK, (h + 1) * DK)
                u = (1.0 - fmin[:, ln]) * sigmoid(-pr[1, lr, ln].astype(F32))
                lg = log_one_minus(u) + sv[gr, ln]
                hi = lg.astype(BF16)
                lo = (lg - hi.astype(F32)).astype(BF16)
                cum = dot(tri2[...], jnp.concatenate([hi, lo], axis=0))
                ref = cum[BLK // 2 - 1 : BLK // 2, :]
                tot = cum[BLK - 1 : BLK, :]
                d = cum - ref
                qraw = pr[0, lr, ln].astype(F32)
                qt = qraw * sigmoid(qraw) * (DK**-0.5) * jnp.exp(d)
                kt = u * jnp.exp(-d)
                runh = run[:, ln]
                qc = (qt * jnp.exp(ref)).astype(BF16)
                qs[gr, ln] = (qt * jnp.exp(ref + runh)).astype(BF16)
                kh = (kt * jnp.exp(tot - ref)).astype(BF16)
                v = pr[2, lr, ln]
                sc = dot(qt.astype(BF16), kt.astype(BF16), NT)
                ri = lax.broadcasted_iota(jnp.int32, (BLK, BLK), 0)
                ci = lax.broadcasted_iota(jnp.int32, (BLK, BLK), 1)
                sc = jnp.where(ri >= ci, sc, 0.0).astype(BF16)
                sh = state[h]
                part[gr, ln] = dot(sc, v) + dot(qc, sh.astype(BF16), NT)
                state[h] = jnp.exp(tot) * sh + dot(v, kh, TN)
                run[:, ln] = runh + tot

        og[rows, :] = pr[3]
        mx[8:, :] = pr[5].astype(F32) * pr[6].astype(F32)
        t = taps[...].astype(F32)
        conv = mx[6 : 6 + tc, :] * t[0:1] + mx[7 : 7 + tc, :] * t[1:2] + mx[8:, :] * t[2:3]
        post = pr[4].astype(F32)
        cv[rows, :] = (post * conv).astype(BF16)

        @pl.when(c == 0)
        def _():
            hd[0:8, :] = conv[0:8]
            hd[8:16, :] = post[0:8]

        mx[0:8, :] = mx[tc : tc + 8, :]
        return carry

    lax.fori_loop(0, chunks, chunk, 0)

    rim[...] = mx[0:8, :]
    for h in range(heads):
        sh = state[h].T
        decay = jnp.exp(run[:, h * DK : (h + 1) * DK])
        for j in range(n_sp):
            st[j, h * own_rows : (h + 1) * own_rows, :] = sh[j * own_rows : (j + 1) * own_rows]
            st[j, heads * own_rows + h : heads * own_rows + h + 1, :] = decay

    def finish(c, carry):
        own(c, True).wait_send()
        own(c, False).wait_send()
        forward(c, True).wait_send()
        forward(c, False).wait_send()
        return carry

    lax.fori_loop(0, chunks, finish, 0)


def pass_states(n_sp, heads, *refs):
    st, start, rim, sin, rim_in = refs[:5]
    got, back, dcol, s1, r1, s2, r2, rs, rr = refs[5:]
    rows = start.shape[0] * start.shape[1]
    own_rows = start.shape[1]
    me = lax.axis_index("sp")
    barrier = pltpu.get_barrier_semaphore()

    def hello(d, carry):
        pl.semaphore_signal(
            barrier, inc=1, device_id={"sp": lax.rem(me + d, n_sp)}, device_id_type=MESH
        )
        return carry

    lax.fori_loop(1, n_sp, hello, 0)
    pl.semaphore_wait(barrier, n_sp - 1)

    def there(d):
        to = lax.rem(me + d, n_sp)
        return pltpu.make_async_remote_copy(
            src_ref=st.at[to],
            dst_ref=got.at[me],
            send_sem=s1.at[d],
            recv_sem=r1.at[d],
            device_id={"sp": to},
            device_id_type=MESH,
        )

    def again(d):
        to = lax.rem(me + d, n_sp)
        return pltpu.make_async_remote_copy(
            src_ref=back.at[to],
            dst_ref=sin.at[me],
            send_sem=s2.at[d],
            recv_sem=r2.at[d],
            device_id={"sp": to},
            device_id_type=MESH,
        )

    def rim_copy():
        return pltpu.make_async_remote_copy(
            src_ref=rim,
            dst_ref=rim_in,
            send_sem=rs,
            recv_sem=rr,
            device_id={"sp": lax.rem(me + 1, n_sp)},
            device_id_type=MESH,
        )

    def each(f):
        def step(d, carry):
            f(d)
            return carry

        lax.fori_loop(1, n_sp, step, 0)

    each(lambda d: there(d).start())
    rim_copy().start()
    got[me] = st[me]
    each(lambda d: there(d).wait_recv())

    hrow = lax.broadcasted_iota(jnp.int32, (rows, DK), 0)
    lane = lax.broadcasted_iota(jnp.int32, (rows, DK), 1)
    pick = lane == me * own_rows + lax.rem(hrow, own_rows)
    for j in range(n_sp):
        dec = jnp.concatenate(
            [
                jnp.broadcast_to(got[j, rows + h : rows + h + 1, :], (own_rows, DK))
                for h in range(heads)
            ],
            axis=0,
        )
        one = jnp.sum(jnp.where(pick, dec, 0.0), axis=1, keepdims=True)
        dcol[j] = jnp.broadcast_to(one, (rows, DK))
    cur = jnp.concatenate([start[h] for h in range(heads)], axis=0)
    for j in range(n_sp):
        back[j] = cur
        cur = dcol[j] * cur + got[j, 0:rows, :]

    each(lambda d: again(d).start())
    sin[me] = back[me]
    each(lambda d: again(d).wait_recv())
    rim_copy().wait_recv()

    def drain(d):
        there(d).wait_send()
        again(d).wait_send()

    each(drain)
    rim_copy().wait_send()


def merge_scatter(n_sp, *refs):
    part, qs, og, cv, hd, rim_in, sin, taps, hgain, wr, wc, ogain, out = refs[:13]
    sb, rec, cvo, po, pp, ra, rb, fl, fr, acc, s_a, s_b, r_a, r_b, s_r, s_l, r_fl, r_fr = refs[13:]
    tokens, width = part.shape
    heads = width // DK
    own_rows = DK // n_sp
    me = lax.axis_index("tp")
    sp = lax.axis_index("sp")
    right, left, opp = lax.rem(me + 1, 4), lax.rem(me + 3, 4), lax.rem(me + 2, 4)
    tb = tokens // 4
    cols = wr.shape[1] // 2

    greet("tp", (left, right))

    for h in range(heads):
        for i in range(n_sp):
            sb[h, i * own_rows : (i + 1) * own_rows, :] = sin[
                i, h * own_rows : (h + 1) * own_rows, :
            ]

    t = taps[...].astype(F32)
    inside = jnp.where(sp == 0, 0.0, 1.0)
    e0 = rim_in[6:7, :] * inside
    e1 = rim_in[7:8, :] * inside
    add0 = e0 * t[0:1] + e1 * t[1:2]
    add1 = e1 * t[0:1]
    ri = lax.broadcasted_iota(jnp.int32, (8, width), 0)
    fix = jnp.where(ri == 0, add0, jnp.where(ri == 1, add1, 0.0))
    head = hd[8:16, :] * (hd[0:8, :] + fix)
    cvo[...] = cv[...]
    cvo[0:16, :] = jnp.concatenate([head, cv[8:16, :].astype(F32)], axis=0).astype(BF16)

    hg = hgain[...].astype(F32)

    def block_rows(owner):
        return pl.ds(pl.multiple_of(owner * tb, 16), tb)

    def mix_heads(owner):
        rows = block_rows(owner)
        for h in range(heads):
            ln = slice(h * DK, (h + 1) * DK)
            o = part[rows, ln] + dot(qs[rows, ln], sb[h].astype(BF16))
            o = o * lax.rsqrt(jnp.mean(o * o, axis=-1, keepdims=True) + EPS) * hg
            g = og[rows, ln].astype(F32)
            rec[rows, ln] = (o * (g * sigmoid(g))).astype(BF16)

    step = 512 if cols % 512 == 0 else cols

    def product(owner, side, put):
        rows = block_rows(owner)

        def one(n, carry):
            cs = pl.ds(pl.multiple_of(n * step, step), step)
            ws = pl.ds(pl.multiple_of(side * cols + n * step, step), step)
            put(cs, dot(rec[rows, :], wr[:, ws]) + dot(cvo[rows, :], wc[:, ws]))
            return carry

        lax.fori_loop(0, cols // step, one, 0)

    def remote(src, dst, ss, rs, to_right):
        return pltpu.make_async_remote_copy(
            src_ref=src,
            dst_ref=dst,
            send_sem=ss,
            recv_sem=rs,
            device_id={"tp": right if to_right else left},
            device_id_type=MESH,
        )

    far_a = remote(po.at[0], ra, s_a, r_a, True)
    far_b = remote(po.at[1], rb, s_b, r_b, False)
    near_r = [remote(pp.at[0, s], fl.at[s], s_r.at[s], r_fl.at[s], True) for s in range(2)]
    near_l = [remote(pp.at[1, s], fr.at[s], s_l.at[s], r_fr.at[s], False) for s in range(2)]

    def store(ref):
        def put(cs, v):
            ref[:, cs] = v.astype(BF16)

        return put

    def store_sum(ref, other):
        def put(cs, v):
            ref[:, cs] = (v + other[:, cs].astype(F32)).astype(BF16)

        return put

    mix_heads(opp)
    product(opp, 0, store(po.at[0]))
    far_a.start()
    product(opp, 1, store(po.at[1]))
    far_b.start()
    mix_heads(right)
    product(right, 1, store(pp.at[0, 1]))
    near_r[1].start()
    mix_heads(left)
    product(left, 0, store(pp.at[1, 0]))
    near_l[0].start()
    mix_heads(me)
    for side in range(2):
        product(me, side, lambda cs, v, side=side: acc.at[side].__setitem__((slice(None), cs), v))
    far_a.wait_recv()
    product(right, 0, store_sum(pp.at[0, 0], ra))
    near_r[0].start()
    far_b.wait_recv()
    product(left, 1, store_sum(pp.at[1, 1], rb))
    near_l[1].start()

    sq = jnp.zeros((tb, 1), F32)
    for side in (1, 0):
        near_r[side].wait_recv()
        near_l[side].wait_recv()
        for n in range(cols // step):
            cs = slice(n * step, (n + 1) * step)
            v = acc[side, :, cs] + fl[side, :, cs].astype(F32) + fr[side, :, cs].astype(F32)
            acc[side, :, cs] = v
            sq = sq + jnp.sum(v * v, axis=1, keepdims=True)
    scale = lax.rsqrt(sq * (1.0 / (2 * cols)) + EPS)
    for side in range(2):
        for n in range(cols // step):
            cs = slice(n * step, (n + 1) * step)
            gs = slice(side * cols + n * step, side * cols + (n + 1) * step)
            out[:, gs] = (acc[side, :, cs] * scale * ogain[:, gs].astype(F32)).astype(BF16)
    far_a.wait_send()
    far_b.wait_send()
    for s in range(2):
        near_r[s].wait_send()
        near_l[s].wait_send()


def solution(mesh):
    n_sp = mesh.shape["sp"]
    vm = pl.BlockSpec(memory_space=pltpu.VMEM)
    hbm = pl.BlockSpec(memory_space=pl.ANY)
    dma = pltpu.SemaphoreType.DMA
    chunks = 4

    def params(cid):
        return pltpu.CompilerParams(
            collective_id=cid, has_side_effects=True, vmem_limit_bytes=VMEM_LIMIT
        )

    def body(x, ing, wq, wf, wval, wog, wpost, wpre, wcv, fmin, surge, taps, hgain, start, wr, wc, ong):
        tokens, width = x.shape
        tc = tokens // chunks
        heads = width // DK
        own_rows = DK // n_sp
        rows = heads * own_rows
        mrows = rows + 8
        sds = jax.ShapeDtypeStruct
        part, qs, og, cv, hd, rim, st = pl.pallas_call(
            lambda *refs: gather_project(chunks, n_sp, *refs),
            out_shape=(
                sds((tokens, width), F32),
                sds((tokens, width), BF16),
                sds((tokens, width), BF16),
                sds((tokens, width), BF16),
                sds((16, width), F32),
                sds((8, width), F32),
                sds((n_sp, mrows, DK), F32),
            ),
            in_specs=[vm, vm, hbm, vm, vm] + [hbm] * 7,
            out_specs=(vm,) * 7,
            scratch_shapes=[
                pltpu.VMEM((tokens, width), BF16),
                pltpu.VMEM((tokens, width), BF16),
                pltpu.VMEM((tokens, width), BF16),
                pltpu.VMEM((tc, 4 * width), BF16),
                pltpu.VMEM((7, 4 * width, width), BF16),
                pltpu.VMEM((tokens, width), F32),
                pltpu.VMEM((7, tc, width), BF16),
                pltpu.VMEM((tc + 8, width), F32),
                pltpu.VMEM((heads, DV, DK), F32),
                pltpu.VMEM((1, width), F32),
                pltpu.VMEM((BLK, 2 * BLK), BF16),
                dma((7, 4)),
                dma,
            ]
            + [dma((chunks,))] * 8,
            compiler_params=params(0),
            name="gather_project",
        )(x, ing.reshape(4, 1, width), surge, fmin.reshape(1, width), taps, wq, wf, wval, wog, wpost, wpre, wcv)

        sin, rim_in = pl.pallas_call(
            lambda *refs: pass_states(n_sp, heads, *refs),
            out_shape=(sds((n_sp, rows, DK), F32), sds((8, width), F32)),
            in_specs=[vm] * 3,
            out_specs=(vm, vm),
            scratch_shapes=[
                pltpu.VMEM((n_sp, mrows, DK), F32),
                pltpu.VMEM((n_sp, rows, DK), F32),
                pltpu.VMEM((n_sp, rows, DK), F32),
            ]
            + [dma((n_sp,))] * 4
            + [dma, dma],
            compiler_params=params(1),
            name="pass_states",
        )(st, start, rim)

        tb = tokens // 4
        cols = wr.shape[1] // 2
        return pl.pallas_call(
            lambda *refs: merge_scatter(n_sp, *refs),
            out_shape=sds((tb, 2 * cols), BF16),
            in_specs=[vm] * 12,
            out_specs=vm,
            scratch_shapes=[
                pltpu.VMEM((heads, DK, DV), F32),
                pltpu.VMEM((tokens, width), BF16),
                pltpu.VMEM((tokens, width), BF16),
                pltpu.VMEM((2, tb, cols), BF16),
                pltpu.VMEM((2, 2, tb, cols), BF16),
                pltpu.VMEM((tb, cols), BF16),
                pltpu.VMEM((tb, cols), BF16),
                pltpu.VMEM((2, tb, cols), BF16),
                pltpu.VMEM((2, tb, cols), BF16),
                pltpu.VMEM((2, tb, cols), F32),
                dma, dma, dma, dma,
                dma((2,)), dma((2,)), dma((2,)), dma((2,)),
            ],
            compiler_params=params(2),
            name="merge_scatter",
        )(part, qs, og, cv, hd, rim_in, sin, taps, hgain.reshape(1, DV), wr, wc, ong.reshape(1, 2 * cols))

    in_specs = (
        P("sp", "tp"),
        P(),
        P(None, "tp"),
        P(None, "tp"),
        P(None, "tp"),
        P(None, "tp"),
        P(None, "tp"),
        P(None, "tp"),
        P(None, "tp"),
        P("tp"),
        P("sp", "tp"),
        P(None, "tp"),
        P(),
        P("tp", "sp", None),
        P("tp", None),
        P("tp", None),
        P(),
    )
    return jax.shard_map(
        body, mesh=mesh, in_specs=in_specs, out_specs=P(("sp", "tp"), None), check_vma=False
    )
```

```python
import jax
import jax.numpy as jnp
from jax import lax
from jax.experimental import pallas as pl
from jax.experimental.pallas import tpu as pltpu
from jax.sharding import PartitionSpec as P

DK = 128
DV = 128
BLK = 64
EPS = 1e-06
MESH = pl.DeviceIdType.MESH
F32 = jnp.float32
BF16 = jnp.bfloat16
VMEM_LIMIT = 62 * 1024 * 1024

NT = (((1,), (1,)), ((), ()))
TN = (((0,), (0,)), ((), ()))


def dot(a, b, dims=None):
    if dims is None:
        return jnp.dot(a, b, preferred_element_type=F32)
    return lax.dot_general(a, b, dims, preferred_element_type=F32)


def sigmoid(v):
    return 1.0 / (1.0 + jnp.exp(-v))


def log_one_minus(u):
    return -u * (1.0 + u * (1 / 2 + u * (1 / 3 + u * (1 / 4 + u * (1 / 5 + u * (1 / 6))))))


def layer(chunks, n_sp, *refs):
    x, gain, surge, fmin, taps, hgain, start, ogain = refs[:8]
    ws = refs[8:15]
    wr_in, wc_in, out = refs[15:18]
    (xl, xr, xo, xn, wv, wr, wc, sv, pr, pd, mx, state, run, tri2, gains) = refs[18:33]
    (part, qs, stf, st, got, dcol, back, sin, rim, rim_in, sb, rec, cvo, accc) = refs[33:47]
    (po, pp, ra, rb, fl, fr, acc) = refs[47:54]
    wsem, msem, s_or, s_ol, s_fr, s_fl, r_l, r_r, r_oa, r_ob = refs[54:64]
    s1, r1, s2, r2, rs, rr = refs[64:70]
    s_a, s_b, r_a, r_b, s_r, s_l, r_fl, r_fr = refs[70:]
    tokens, width = x.shape
    full = 4 * width
    tc = tokens // chunks
    half = tc // 2
    heads = width // DK
    own_rows = DK // n_sp
    srows = heads * own_rows
    tb = tokens // 4
    cols = full // 2
    me = lax.axis_index("tp")
    sp = lax.axis_index("sp")
    right, left, opp = lax.rem(me + 1, 4), lax.rem(me + 3, 4), lax.rem(me + 2, 4)
    srcs = (me, left, right, opp)

    first, later = [], []
    for k in range(7):
        for r in range(4):
            rows = pl.ds(pl.multiple_of(srcs[r] * width, width), width)
            copy = pltpu.make_async_copy(
                ws[k].at[rows, :], wv.at[k, pl.ds(r * width, width), :], wsem.at[k, r]
            )
            (first if k < 3 else later).append(copy)
    first.append(pltpu.make_async_copy(surge, sv, msem.at[0]))
    later.append(pltpu.make_async_copy(wr_in, wr, msem.at[1]))
    later.append(pltpu.make_async_copy(wc_in, wc, msem.at[2]))
    for copy in first + later:
        copy.start()

    barrier = pltpu.get_barrier_semaphore()
    for peer in (left, right):
        pl.semaphore_signal(barrier, inc=1, device_id={"tp": peer}, device_id_type=MESH)

    def each(f):
        def step(d, carry):
            f(d)
            return carry

        lax.fori_loop(1, n_sp, step, 0)

    each(
        lambda d: pl.semaphore_signal(
            barrier, inc=1, device_id={"sp": lax.rem(sp + d, n_sp)}, device_id_type=MESH
        )
    )
    pl.semaphore_wait(barrier, 2 + n_sp - 1)

    def beside(src, dst, ss, rs, to_right):
        return pltpu.make_async_remote_copy(
            src_ref=src,
            dst_ref=dst,
            send_sem=ss,
            recv_sem=rs,
            device_id={"tp": right if to_right else left},
            device_id_type=MESH,
        )

    def along(src, dst, ss, rs, to):
        return pltpu.make_async_remote_copy(
            src_ref=src,
            dst_ref=dst,
            send_sem=ss,
            recv_sem=rs,
            device_id={"sp": to},
            device_id_type=MESH,
        )

    def rows_of(c, size, off=0):
        return pl.ds(pl.multiple_of(c * tc + off, 16), size)

    def own(c, to_right):
        rows = rows_of(c, tc)
        return beside(
            x.at[rows, :],
            (xl if to_right else xr).at[rows, :],
            (s_or if to_right else s_ol).at[c],
            (r_l if to_right else r_r).at[c],
            to_right,
        )

    def forward(c, to_right):
        rows = rows_of(c, half, 0 if to_right else half)
        return beside(
            (xl if to_right else xr).at[rows, :],
            xo.at[rows, :],
            (s_fr if to_right else s_fl).at[c],
            (r_oa if to_right else r_ob).at[c],
            to_right,
        )

    def pass_on(c):
        own(c, True).wait_recv()
        forward(c, True).start()
        own(c, False).wait_recv()
        forward(c, False).start()

    lead = min(2, chunks)
    for c in range(lead):
        own(c, True).start()
        own(c, False).start()

    state[...] = jnp.zeros_like(state)
    run[...] = jnp.zeros_like(run)
    gains[...] = gain[...].astype(F32).reshape(1, full)
    row = lax.broadcasted_iota(jnp.int32, (BLK, 2 * BLK), 0)
    col = lax.broadcasted_iota(jnp.int32, (BLK, 2 * BLK), 1)
    tri2[...] = jnp.where(row >= lax.rem(col, BLK), 1.0, 0.0).astype(BF16)

    pass_on(0)
    if chunks > lead:
        own(lead, True).start()
        own(lead, False).start()
    for copy in first:
        copy.wait()

    def chunk(c, carry):
        @pl.when(c + 1 < chunks)
        def _():
            pass_on(c + 1)

        @pl.when(c + 1 + lead < chunks)
        def _():
            own(c + 1 + lead, True).start()
            own(c + 1 + lead, False).start()

        forward(c, True).wait_recv()
        forward(c, False).wait_recv()

        rows = rows_of(c, tc)
        total = jnp.zeros((tc, 1), F32)
        for piece in (x, xl, xr, xo):
            v = piece[rows, :].astype(F32)
            total = total + jnp.sum(v * v, axis=1, keepdims=True)
        scale = lax.rsqrt(total * (1.0 / full) + EPS)
        for r, piece in enumerate((x, xl, xr, xo)):
            g = gains[:, pl.ds(pl.multiple_of(srcs[r] * width, width), width)]
            v = piece[rows, :].astype(F32) * scale * g
            xn[rows, r * width : (r + 1) * width] = v.astype(BF16)

        def project(k, carry):
            pr[k] = dot(xn[rows, :], wv[k]).astype(BF16)
            return carry

        lax.fori_loop(0, 3, project, 0)

        for b in range(tc // BLK):
            lr = slice(b * BLK, (b + 1) * BLK)
            gr = rows_of(c, BLK, b * BLK)
            for h in range(heads):
                ln = slice(h * DK, (h + 1) * DK)
                u = (1.0 - fmin[:, ln]) * sigmoid(-pr[1, lr, ln].astype(F32))
                lg = log_one_minus(u) + sv[gr, ln]
                hi = lg.astype(BF16)
                lo = (lg - hi.astype(F32)).astype(BF16)
                cum = dot(tri2[...], jnp.concatenate([hi, lo], axis=0))
                ref = cum[BLK // 2 - 1 : BLK // 2, :]
                tot = cum[BLK - 1 : BLK, :]
                d = cum - ref
                qraw = pr[0, lr, ln].astype(F32)
                qt = qraw * sigmoid(qraw) * (DK**-0.5) * jnp.exp(d)
                kt = u * jnp.exp(-d)
                runh = run[:, ln]
                qc = (qt * jnp.exp(ref)).astype(BF16)
                qs[gr, ln] = (qt * jnp.exp(ref + runh)).astype(BF16)
                kh = (kt * jnp.exp(tot - ref)).astype(BF16)
                v = pr[2, lr, ln]
                sc = dot(qt.astype(BF16), kt.astype(BF16), NT)
                ri = lax.broadcasted_iota(jnp.int32, (BLK, BLK), 0)
                ci = lax.broadcasted_iota(jnp.int32, (BLK, BLK), 1)
                sc = jnp.where(ri >= ci, sc, 0.0).astype(BF16)
                sh = state[h]
                part[gr, ln] = dot(sc, v) + dot(qc, sh.astype(BF16), NT)
                state[h] = jnp.exp(tot) * sh + dot(v, kh, TN)
                run[:, ln] = runh + tot
        return carry

    lax.fori_loop(0, chunks, chunk, 0)

    for h in range(heads):
        sh = state[h].T
        decay = jnp.exp(run[:, h * DK : (h + 1) * DK])
        top = decay.astype(BF16).astype(F32)
        for j in range(n_sp):
            stf[j, h * own_rows : (h + 1) * own_rows, :] = sh[j * own_rows : (j + 1) * own_rows]
            stf[j, srows + h : srows + h + 1, :] = top
            stf[j, srows + heads + h : srows + heads + h + 1, :] = decay - top
    for j in range(n_sp):
        st[j] = stf[j].astype(BF16)

    def there(d):
        to = lax.rem(sp + d, n_sp)
        return along(st.at[to], got.at[sp], s1.at[d], r1.at[d], to)

    def again(d):
        to = lax.rem(sp + d, n_sp)
        return along(back.at[to], sin.at[sp], s2.at[d], r2.at[d], to)

    def rim_copy():
        return along(rim, rim_in, rs, rr, lax.rem(sp + 1, n_sp))

    each(lambda d: there(d).start())
    got[sp] = st[sp]

    for copy in later:
        copy.wait()

    def wide(k, carry):
        pd[k] = dot(xn[...], wv[k + 3]).astype(BF16)
        return carry

    lax.fori_loop(0, 2, wide, 0)
    mx[0:8, :] = jnp.zeros((8, width), F32)
    piece = tokens // 8

    def mixing(i, carry):
        rows = pl.ds(pl.multiple_of(i * piece, 16), piece)
        mx[pl.ds(pl.multiple_of(i * piece + 8, 8), piece), :] = pd[0, rows, :].astype(F32) * pd[
            1, rows, :
        ].astype(F32)
        return carry

    lax.fori_loop(0, 8, mixing, 0)
    rim[...] = mx[tokens : tokens + 8, :]
    rim_copy().start()

    each(lambda d: there(d).wait_recv())
    hrow = lax.broadcasted_iota(jnp.int32, (srows, DK), 0)
    lane = lax.broadcasted_iota(jnp.int32, (srows, DK), 1)
    pick = lane == sp * own_rows + lax.rem(hrow, own_rows)
    for j in range(n_sp):
        gj = got[j].astype(F32)
        both = gj[srows : srows + heads] + gj[srows + heads : srows + 2 * heads]
        dec = jnp.concatenate(
            [jnp.broadcast_to(both[h : h + 1, :], (own_rows, DK)) for h in range(heads)],
            axis=0,
        )
        one = jnp.sum(jnp.where(pick, dec, 0.0), axis=1, keepdims=True)
        dcol[j] = jnp.broadcast_to(one, (srows, DK))
    cur = jnp.concatenate([start[h] for h in range(heads)], axis=0)
    for j in range(n_sp):
        back[j] = cur.astype(BF16)
        cur = dcol[j] * cur + got[j].astype(F32)[0:srows]

    each(lambda d: again(d).start())
    sin[sp] = back[sp]

    lax.fori_loop(2, 4, wide, 0)
    rim_copy().wait_recv()
    inside = jnp.where(sp == 0, 0.0, 1.0)
    mx[0:8, :] = rim_in[...] * inside
    t = taps[...].astype(F32)

    def convolve(i, carry):
        rows = pl.ds(pl.multiple_of(i * piece, 16), piece)
        v = mx[pl.ds(pl.multiple_of(i * piece, 8), piece + 8), :]
        conv = v[6 : 6 + piece] * t[0:1] + v[7 : 7 + piece] * t[1:2] + v[8:] * t[2:3]
        cvo[rows, :] = (pd[2, rows, :].astype(F32) * conv).astype(BF16)
        return carry

    lax.fori_loop(0, 8, convolve, 0)

    step = 512 if cols % 512 == 0 else cols

    def conv_part(n, carry):
        cs = pl.ds(pl.multiple_of(n * step, step), step)
        accc[:, cs] = dot(cvo[...], wc[:, cs])
        return carry

    lax.fori_loop(0, full // step, conv_part, 0)

    each(lambda d: again(d).wait_recv())
    for i in range(n_sp):
        si = sin[i].astype(F32)
        for h in range(heads):
            sb[h, i * own_rows : (i + 1) * own_rows, :] = si[h * own_rows : (h + 1) * own_rows, :]

    hg = hgain[...].astype(F32)

    def block_rows(owner):
        return pl.ds(pl.multiple_of(owner * tb, 16), tb)

    def mix_heads(owner):
        rows = block_rows(owner)
        for h in range(heads):
            ln = slice(h * DK, (h + 1) * DK)
            o = part[rows, ln] + dot(qs[rows, ln], sb[h].astype(BF16))
            o = o * lax.rsqrt(jnp.mean(o * o, axis=-1, keepdims=True) + EPS) * hg
            g = pd[3, rows, ln].astype(F32)
            rec[rows, ln] = (o * (g * sigmoid(g))).astype(BF16)

    def product(owner, side, put):
        rows = block_rows(owner)

        def one(n, carry):
            cs = pl.ds(pl.multiple_of(n * step, step), step)
            ns = pl.ds(pl.multiple_of(side * cols + n * step, step), step)
            put(cs, dot(rec[rows, :], wr[:, ns]) + accc[rows, ns])
            return carry

        lax.fori_loop(0, cols // step, one, 0)

    far_a = beside(po.at[0], ra, s_a, r_a, True)
    far_b = beside(po.at[1], rb, s_b, r_b, False)
    near_r = [beside(pp.at[0, s], fl.at[s], s_r.at[s], r_fl.at[s], True) for s in range(2)]
    near_l = [beside(pp.at[1, s], fr.at[s], s_l.at[s], r_fr.at[s], False) for s in range(2)]

    def store(ref):
        def put(cs, v):
            ref[:, cs] = v.astype(BF16)

        return put

    def store_sum(ref, other):
        def put(cs, v):
            ref[:, cs] = (v + other[:, cs].astype(F32)).astype(BF16)

        return put

    def keep(side):
        def put(cs, v):
            acc[side, :, cs] = v

        return put

    mix_heads(opp)
    product(opp, 0, store(po.at[0]))
    far_a.start()
    product(opp, 1, store(po.at[1]))
    far_b.start()
    mix_heads(right)
    product(right, 1, store(pp.at[0, 1]))
    near_r[1].start()
    mix_heads(left)
    product(left, 0, store(pp.at[1, 0]))
    near_l[0].start()
    mix_heads(me)
    for side in range(2):
        product(me, side, keep(side))
    far_a.wait_recv()
    product(right, 0, store_sum(pp.at[0, 0], ra))
    near_r[0].start()
    far_b.wait_recv()
    product(left, 1, store_sum(pp.at[1, 1], rb))
    near_l[1].start()

    sq = jnp.zeros((tb, 1), F32)
    for side in (1, 0):
        near_r[side].wait_recv()
        near_l[side].wait_recv()
        for n in range(cols // step):
            cs = slice(n * step, (n + 1) * step)
            v = acc[side, :, cs] + fl[side, :, cs].astype(F32) + fr[side, :, cs].astype(F32)
            acc[side, :, cs] = v
            sq = sq + jnp.sum(v * v, axis=1, keepdims=True)
    scale = lax.rsqrt(sq * (1.0 / full) + EPS)
    gains[...] = ogain[...].astype(F32).reshape(1, full)
    for side in range(2):
        for n in range(cols // step):
            cs = slice(n * step, (n + 1) * step)
            gs = slice(side * cols + n * step, side * cols + (n + 1) * step)
            out[:, gs] = (acc[side, :, cs] * scale * gains[:, gs]).astype(BF16)

    def finish(c, carry):
        own(c, True).wait_send()
        own(c, False).wait_send()
        forward(c, True).wait_send()
        forward(c, False).wait_send()
        return carry

    lax.fori_loop(0, chunks, finish, 0)

    def drain(d):
        there(d).wait_send()
        again(d).wait_send()

    each(drain)
    rim_copy().wait_send()
    far_a.wait_send()
    far_b.wait_send()
    for s in range(2):
        near_r[s].wait_send()
        near_l[s].wait_send()


def solution(mesh):
    n_sp = mesh.shape["sp"]
    vm = pl.BlockSpec(memory_space=pltpu.VMEM)
    hbm = pl.BlockSpec(memory_space=pl.ANY)
    dma = pltpu.SemaphoreType.DMA
    chunks = 4

    def body(x, ing, wq, wf, wval, wog, wpost, wpre, wcv, fmin, surge, taps, hgain, start, wr, wc, ong):
        tokens, width = x.shape
        tc = tokens // chunks
        heads = width // DK
        own_rows = DK // n_sp
        rows = heads * own_rows
        mrows = rows + 2 * heads
        tb = tokens // 4
        full = 4 * width
        cols = full // 2
        v = pltpu.VMEM
        return pl.pallas_call(
            lambda *refs: layer(chunks, n_sp, *refs),
            out_shape=jax.ShapeDtypeStruct((tb, full), BF16),
            in_specs=[vm, vm, hbm, vm, vm, vm, vm, vm] + [hbm] * 9,
            out_specs=vm,
            scratch_shapes=[
                v((tokens, width), BF16),
                v((tokens, width), BF16),
                v((tokens, width), BF16),
                v((tokens, full), BF16),
                v((7, full, width), BF16),
                v((width, full), BF16),
                v((width, full), BF16),
                v((tokens, width), F32),
                v((3, tc, width), BF16),
                v((4, tokens, width), BF16),
                v((tokens + 8, width), F32),
                v((heads, DV, DK), F32),
                v((1, width), F32),
                v((BLK, 2 * BLK), BF16),
                v((1, full), F32),
                v((tokens, width), F32),
                v((tokens, width), BF16),
                v((n_sp, mrows, DK), F32),
                v((n_sp, mrows, DK), BF16),
                v((n_sp, mrows, DK), BF16),
                v((n_sp, rows, DK), F32),
                v((n_sp, rows, DK), BF16),
                v((n_sp, rows, DK), BF16),
                v((8, width), F32),
                v((8, width), F32),
                v((heads, DK, DV), F32),
                v((tokens, width), BF16),
                v((tokens, width), BF16),
                v((tokens, full), F32),
                v((2, tb, cols), BF16),
                v((2, 2, tb, cols), BF16),
                v((tb, cols), BF16),
                v((tb, cols), BF16),
                v((2, tb, cols), BF16),
                v((2, tb, cols), BF16),
                v((2, tb, cols), F32),
                dma((7, 4)),
                dma((3,)),
            ]
            + [dma((chunks,))] * 8
            + [dma((n_sp,))] * 4
            + [dma] * 6
            + [dma((2,))] * 4,
            compiler_params=pltpu.CompilerParams(
                collective_id=0, has_side_effects=True, vmem_limit_bytes=VMEM_LIMIT
            ),
            name="layer",
        )(x, ing, surge, fmin.reshape(1, width), taps, hgain.reshape(1, DV), start, ong,
          wq, wf, wval, wpre, wcv, wpost, wog, wr, wc)

    in_specs = (
        P("sp", "tp"),
        P(),
        P(None, "tp"),
        P(None, "tp"),
        P(None, "tp"),
        P(None, "tp"),
        P(None, "tp"),
        P(None, "tp"),
        P(None, "tp"),
        P("tp"),
        P("sp", "tp"),
        P(None, "tp"),
        P(),
        P("tp", "sp", None),
        P("tp", None),
        P("tp", None),
        P(),
    )
    return jax.shard_map(
        body, mesh=mesh, in_specs=in_specs, out_specs=P(("sp", "tp"), None), check_vma=False
    )
```

```python
import jax
import jax.numpy as jnp
from jax import lax
from jax.experimental import pallas as pl
from jax.experimental.pallas import tpu as pltpu
from jax.sharding import PartitionSpec as P

DK = 128
DV = 128
BLK = 64
EPS = 1e-06
MESH = pl.DeviceIdType.MESH
F32 = jnp.float32
BF16 = jnp.bfloat16
VMEM_LIMIT = 62 * 1024 * 1024

NT = (((1,), (1,)), ((), ()))
TN = (((0,), (0,)), ((), ()))


def dot(a, b, dims=None):
    if dims is None:
        return jnp.dot(a, b, preferred_element_type=F32)
    return lax.dot_general(a, b, dims, preferred_element_type=F32)


def sigmoid(v):
    return lax.logistic(v)


def log_one_minus(u):
    return -u * (1.0 + u * (1 / 2 + u * (1 / 3 + u * (1 / 4 + u * (1 / 5 + u * (1 / 6))))))


def layer(chunks, n_sp, *refs):
    x, gain, surge, fmin, taps, hgain, start, ogain = refs[:8]
    ws = refs[8:15]
    wr_in, wc_in, out = refs[15:18]
    (xl, xr, xo, xn, wv, wr, wc, sv, pr, pd, mx, state, run, tri2, gains) = refs[18:33]
    (part3, scales, part, qs, stf, st, got, dcol, back, sin, rim, rim_in, sb, rec, cvo, accc) = refs[33:49]
    (po, pp, ra, rb, fl, fr, acc) = refs[49:56]
    known, wsem, msem, s_or, s_ol, s_fr, s_fl, r_l, r_r, r_oa, r_ob = refs[56:67]
    s1, r1, s2, r2, rs, rr = refs[67:73]
    s_a, s_b, r_a, r_b, s_r, s_l, r_fl, r_fr = refs[73:]
    tokens, width = x.shape
    full = 4 * width
    tc = tokens // chunks
    parts = 2 * chunks
    tm = tokens // parts
    half = tm // 2
    heads = width // DK
    own_rows = DK // n_sp
    srows = heads * own_rows
    tb = tokens // 4
    cols = full // 2
    me = lax.axis_index("tp")
    sp = lax.axis_index("sp")
    right, left, opp = lax.rem(me + 1, 4), lax.rem(me + 3, 4), lax.rem(me + 2, 4)
    srcs = (me, left, right, opp)

    first, early, later = [], [], []
    for k in range(7):
        for r in range(4):
            rows = pl.ds(pl.multiple_of(srcs[r] * width, width), width)
            copy = pltpu.make_async_copy(
                ws[k].at[rows, :], wv.at[k, pl.ds(r * width, width), :], wsem.at[k, r]
            )
            (early if r == 0 else first if k < 3 else later).append(copy)
    first.append(pltpu.make_async_copy(surge, sv, msem.at[0]))
    later.append(pltpu.make_async_copy(wr_in, wr, msem.at[1]))
    later.append(pltpu.make_async_copy(wc_in, wc, msem.at[2]))
    for copy in early + first + later:
        copy.start()

    barrier = pltpu.get_barrier_semaphore()
    for peer in (left, right):
        pl.semaphore_signal(barrier, inc=1, device_id={"tp": peer}, device_id_type=MESH)

    def each(f):
        def step(d, carry):
            f(d)
            return carry

        lax.fori_loop(1, n_sp, step, 0)

    def tell(sem, d):
        for to in (lax.rem(sp + d, n_sp), lax.rem(sp + n_sp - d, n_sp)):
            pl.semaphore_signal(sem, inc=1, device_id={"sp": to}, device_id_type=MESH)

    tell(barrier, 1)
    pl.semaphore_wait(barrier, 4)
    rounds = n_sp.bit_length() - 2
    tell(known.at[0], 1)

    def beside(src, dst, ss, rs, to_right):
        return pltpu.make_async_remote_copy(
            src_ref=src,
            dst_ref=dst,
            send_sem=ss,
            recv_sem=rs,
            device_id={"tp": right if to_right else left},
            device_id_type=MESH,
        )

    def along(src, dst, ss, rs, to):
        return pltpu.make_async_remote_copy(
            src_ref=src,
            dst_ref=dst,
            send_sem=ss,
            recv_sem=rs,
            device_id={"sp": to},
            device_id_type=MESH,
        )

    def rows_of(c, size, off=0):
        return pl.ds(pl.multiple_of(c * tc + off, 16), size)

    def own(c, to_right):
        rows = pl.ds(pl.multiple_of(c * tm, 16), tm)
        return beside(
            x.at[rows, :],
            (xl if to_right else xr).at[rows, :],
            (s_or if to_right else s_ol).at[c],
            (r_l if to_right else r_r).at[c],
            to_right,
        )

    def forward(c, to_right):
        rows = pl.ds(pl.multiple_of(c * tm + (0 if to_right else half), 16), half)
        return beside(
            (xl if to_right else xr).at[rows, :],
            xo.at[rows, :],
            (s_fr if to_right else s_fl).at[c],
            (r_oa if to_right else r_ob).at[c],
            to_right,
        )

    def pass_on(c):
        own(c, True).wait_recv()
        forward(c, True).start()
        own(c, False).wait_recv()
        forward(c, False).start()

    def send(c):
        own(c, True).start()
        own(c, False).start()

    send(0)
    send(1)

    state[...] = jnp.zeros_like(state)
    run[...] = jnp.zeros_like(run)
    gains[...] = gain[...].astype(F32).reshape(1, full)
    row = lax.broadcasted_iota(jnp.int32, (BLK, 2 * BLK), 0)
    col = lax.broadcasted_iota(jnp.int32, (BLK, 2 * BLK), 1)
    tri2[...] = jnp.where(row >= lax.rem(col, BLK), 1.0, 0.0).astype(BF16)

    xn[:, 0:width] = (x[...].astype(F32) * gains[:, pl.ds(pl.multiple_of(me * width, width), width)]).astype(BF16)
    for copy in early:
        copy.wait()

    def own_wide(k, carry):
        cs = pl.ds(pl.multiple_of(k * width, width), width)
        accc[:, cs] = dot(xn[:, 0:width], wv[k + 3, 0:width, :])
        return carry

    def own_narrow(k, carry):
        part3[k] = dot(xn[:, 0:width], wv[k, 0:width, :])
        return carry

    lax.fori_loop(0, 3, own_narrow, 0)
    pass_on(0)
    send(2)
    lax.fori_loop(0, 4, own_wide, 0)
    pass_on(1)
    send(3)
    for copy in first:
        copy.wait()

    def chunk(c, carry):
        def relay(m):
            @pl.when(m < parts)
            def _():
                pass_on(m)

            @pl.when(m + 2 < parts)
            def _():
                send(m + 2)

        relay(2 * c + 2)
        for m in range(2):
            forward(2 * c + m, True).wait_recv()
            forward(2 * c + m, False).wait_recv()

        rows = rows_of(c, tc)
        total = jnp.zeros((tc, 1), F32)
        for piece in (x, xl, xr, xo):
            v = piece[rows, :].astype(F32)
            total = total + jnp.sum(v * v, axis=1, keepdims=True)
        scale = lax.rsqrt(total * (1.0 / full) + EPS)
        scales[rows, :] = jnp.broadcast_to(scale, (tc, DK))
        for r, piece in ((1, xl), (2, xr), (3, xo)):
            g = gains[:, pl.ds(pl.multiple_of(srcs[r] * width, width), width)]
            xn[rows, r * width : (r + 1) * width] = (piece[rows, :].astype(F32) * g).astype(BF16)

        def project(k, carry):
            total = dot(xn[rows, width:], wv[k, width:, :]) + part3[k, rows, :]
            pr[k] = (total * scales[rows, 0:1]).astype(BF16)
            return carry

        lax.fori_loop(0, 3, project, 0)
        relay(2 * c + 3)

        for b in range(tc // BLK):
            lr = slice(b * BLK, (b + 1) * BLK)
            gr = rows_of(c, BLK, b * BLK)
            for h in range(heads):
                ln = slice(h * DK, (h + 1) * DK)
                u = (1.0 - fmin[:, ln]) * sigmoid(-pr[1, lr, ln].astype(F32))
                lg = log_one_minus(u) + sv[gr, ln]
                hi = lg.astype(BF16)
                lo = (lg - hi.astype(F32)).astype(BF16)
                cum = dot(tri2[...], jnp.concatenate([hi, lo], axis=0))
                ref = cum[BLK // 2 - 1 : BLK // 2, :]
                tot = cum[BLK - 1 : BLK, :]
                d = cum - ref
                qraw = pr[0, lr, ln].astype(F32)
                qt = qraw * sigmoid(qraw) * (DK**-0.5) * jnp.exp(d)
                kt = u * jnp.exp(-d)
                runh = run[:, ln]
                qc = (qt * jnp.exp(ref)).astype(BF16)
                qs[gr, ln] = (qt * jnp.exp(ref + runh)).astype(BF16)
                kh = (kt * jnp.exp(tot - ref)).astype(BF16)
                v = pr[2, lr, ln]
                sc = dot(qt.astype(BF16), kt.astype(BF16), NT)
                ri = lax.broadcasted_iota(jnp.int32, (BLK, BLK), 0)
                ci = lax.broadcasted_iota(jnp.int32, (BLK, BLK), 1)
                sc = jnp.where(ri >= ci, sc, 0.0).astype(BF16)
                sh = state[h]
                part[gr, ln] = dot(sc, v) + dot(qc, sh.astype(BF16), NT)
                state[h] = jnp.exp(tot) * sh + dot(v, kh, TN)
                run[:, ln] = runh + tot
        for k in range(rounds):

            @pl.when(c == k)
            def _():
                pl.semaphore_wait(known.at[k], 2)
                if k + 1 < rounds:
                    tell(known.at[k + 1], 2 ** (k + 1))

        return carry

    lax.fori_loop(0, chunks, chunk, 0)

    for h in range(heads):
        sh = state[h].T
        decay = jnp.exp(run[:, h * DK : (h + 1) * DK])
        top = decay.astype(BF16).astype(F32)
        for j in range(n_sp):
            stf[j, h * own_rows : (h + 1) * own_rows, :] = sh[j * own_rows : (j + 1) * own_rows]
            stf[j, srows + h : srows + h + 1, :] = top
            stf[j, srows + heads + h : srows + heads + h + 1, :] = decay - top
    for j in range(n_sp):
        st[j] = stf[j].astype(BF16)

    def there(d):
        to = lax.rem(sp + d, n_sp)
        return along(st.at[to], got.at[sp], s1.at[d], r1.at[d], to)

    def again(d):
        to = lax.rem(sp + d, n_sp)
        return along(back.at[to], sin.at[sp], s2.at[d], r2.at[d], to)

    def rim_copy():
        return along(rim, rim_in, rs, rr, lax.rem(sp + 1, n_sp))

    each(lambda d: there(d).start())
    got[sp] = st[sp]

    for copy in later:
        copy.wait()

    def wide(k, carry):
        cs = pl.ds(pl.multiple_of(k * width, width), width)
        total = dot(xn[:, width:], wv[k + 3, width:, :]) + accc[:, cs]
        pd[k] = (total * scales[:, 0:1]).astype(BF16)
        return carry

    lax.fori_loop(0, 2, wide, 0)
    mx[0:8, :] = jnp.zeros((8, width), F32)
    piece = tokens // 8

    def mixing(i, carry):
        rows = pl.ds(pl.multiple_of(i * piece, 16), piece)
        mx[pl.ds(pl.multiple_of(i * piece + 8, 8), piece), :] = pd[0, rows, :].astype(F32) * pd[
            1, rows, :
        ].astype(F32)
        return carry

    lax.fori_loop(0, 8, mixing, 0)
    rim[...] = mx[tokens : tokens + 8, :]
    rim_copy().start()

    each(lambda d: there(d).wait_recv())
    hrow = lax.broadcasted_iota(jnp.int32, (srows, DK), 0)
    lane = lax.broadcasted_iota(jnp.int32, (srows, DK), 1)
    pick = lane == sp * own_rows + lax.rem(hrow, own_rows)
    for j in range(n_sp):
        gj = got[j].astype(F32)
        both = gj[srows : srows + heads] + gj[srows + heads : srows + 2 * heads]
        dec = jnp.concatenate(
            [jnp.broadcast_to(both[h : h + 1, :], (own_rows, DK)) for h in range(heads)],
            axis=0,
        )
        one = jnp.sum(jnp.where(pick, dec, 0.0), axis=1, keepdims=True)
        dcol[j] = jnp.broadcast_to(one, (srows, DK))
    cur = jnp.concatenate([start[h] for h in range(heads)], axis=0)
    for j in range(n_sp):
        back[j] = cur.astype(BF16)
        cur = dcol[j] * cur + got[j].astype(F32)[0:srows]

    each(lambda d: again(d).start())
    sin[sp] = back[sp]

    lax.fori_loop(2, 4, wide, 0)
    rim_copy().wait_recv()
    inside = jnp.where(sp == 0, 0.0, 1.0)
    mx[0:8, :] = rim_in[...] * inside
    t = taps[...].astype(F32)

    def convolve(i, carry):
        rows = pl.ds(pl.multiple_of(i * piece, 16), piece)
        v = mx[pl.ds(pl.multiple_of(i * piece, 8), piece + 8), :]
        conv = v[6 : 6 + piece] * t[0:1] + v[7 : 7 + piece] * t[1:2] + v[8:] * t[2:3]
        cvo[rows, :] = (pd[2, rows, :].astype(F32) * conv).astype(BF16)
        return carry

    lax.fori_loop(0, 8, convolve, 0)

    step = 512 if cols % 512 == 0 else cols

    def conv_part(n, carry):
        cs = pl.ds(pl.multiple_of(n * step, step), step)
        accc[:, cs] = dot(cvo[...], wc[:, cs])
        return carry

    lax.fori_loop(0, full // step, conv_part, 0)

    each(lambda d: again(d).wait_recv())
    for i in range(n_sp):
        si = sin[i].astype(F32)
        for h in range(heads):
            sb[h, i * own_rows : (i + 1) * own_rows, :] = si[h * own_rows : (h + 1) * own_rows, :]

    hg = hgain[...].astype(F32)

    def block_rows(owner):
        return pl.ds(pl.multiple_of(owner * tb, 16), tb)

    def mix_heads(owner):
        rows = block_rows(owner)
        for h in range(heads):
            ln = slice(h * DK, (h + 1) * DK)
            o = part[rows, ln] + dot(qs[rows, ln], sb[h].astype(BF16))
            o = o * lax.rsqrt(jnp.mean(o * o, axis=-1, keepdims=True) + EPS) * hg
            g = pd[3, rows, ln].astype(F32)
            rec[rows, ln] = (o * (g * sigmoid(g))).astype(BF16)

    def product(owner, side, put):
        rows = block_rows(owner)

        def one(n, carry):
            cs = pl.ds(pl.multiple_of(n * step, step), step)
            ns = pl.ds(pl.multiple_of(side * cols + n * step, step), step)
            put(cs, dot(rec[rows, :], wr[:, ns]) + accc[rows, ns])
            return carry

        lax.fori_loop(0, cols // step, one, 0)

    far_a = beside(po.at[0], ra, s_a, r_a, True)
    far_b = beside(po.at[1], rb, s_b, r_b, False)
    near_r = [beside(pp.at[0, s], fl.at[s], s_r.at[s], r_fl.at[s], True) for s in range(2)]
    near_l = [beside(pp.at[1, s], fr.at[s], s_l.at[s], r_fr.at[s], False) for s in range(2)]

    def store(ref):
        def put(cs, v):
            ref[:, cs] = v.astype(BF16)

        return put

    def store_sum(ref, other):
        def put(cs, v):
            ref[:, cs] = (v + other[:, cs].astype(F32)).astype(BF16)

        return put

    def keep(side):
        def put(cs, v):
            acc[side, :, cs] = v

        return put

    mix_heads(opp)
    product(opp, 0, store(po.at[0]))
    far_a.start()
    product(opp, 1, store(po.at[1]))
    far_b.start()
    mix_heads(right)
    product(right, 1, store(pp.at[0, 1]))
    near_r[1].start()
    mix_heads(left)
    product(left, 0, store(pp.at[1, 0]))
    near_l[0].start()
    mix_heads(me)
    for side in range(2):
        product(me, side, keep(side))
    far_a.wait_recv()
    product(right, 0, store_sum(pp.at[0, 0], ra))
    near_r[0].start()
    far_b.wait_recv()
    product(left, 1, store_sum(pp.at[1, 1], rb))
    near_l[1].start()

    sq = jnp.zeros((tb, 1), F32)
    for side in (1, 0):
        near_r[side].wait_recv()
        near_l[side].wait_recv()
        for n in range(cols // step):
            cs = slice(n * step, (n + 1) * step)
            v = acc[side, :, cs] + fl[side, :, cs].astype(F32) + fr[side, :, cs].astype(F32)
            acc[side, :, cs] = v
            sq = sq + jnp.sum(v * v, axis=1, keepdims=True)
    scale = lax.rsqrt(sq * (1.0 / full) + EPS)
    gains[...] = ogain[...].astype(F32).reshape(1, full)
    for side in range(2):
        for n in range(cols // step):
            cs = slice(n * step, (n + 1) * step)
            gs = slice(side * cols + n * step, side * cols + (n + 1) * step)
            out[:, gs] = (acc[side, :, cs] * scale * gains[:, gs]).astype(BF16)

    def finish(c, carry):
        own(c, True).wait_send()
        own(c, False).wait_send()
        forward(c, True).wait_send()
        forward(c, False).wait_send()
        return carry

    lax.fori_loop(0, parts, finish, 0)

    def drain(d):
        there(d).wait_send()
        again(d).wait_send()

    each(drain)
    rim_copy().wait_send()
    far_a.wait_send()
    far_b.wait_send()
    for s in range(2):
        near_r[s].wait_send()
        near_l[s].wait_send()


def solution(mesh):
    n_sp = mesh.shape["sp"]
    vm = pl.BlockSpec(memory_space=pltpu.VMEM)
    hbm = pl.BlockSpec(memory_space=pl.ANY)
    dma = pltpu.SemaphoreType.DMA
    chunks = 4

    def body(x, ing, wq, wf, wval, wog, wpost, wpre, wcv, fmin, surge, taps, hgain, start, wr, wc, ong):
        tokens, width = x.shape
        tc = tokens // chunks
        heads = width // DK
        own_rows = DK // n_sp
        rows = heads * own_rows
        mrows = rows + 2 * heads
        tb = tokens // 4
        full = 4 * width
        cols = full // 2
        v = pltpu.VMEM
        return pl.pallas_call(
            lambda *refs: layer(chunks, n_sp, *refs),
            out_shape=jax.ShapeDtypeStruct((tb, full), BF16),
            in_specs=[vm, vm, hbm, vm, vm, vm, vm, vm] + [hbm] * 9,
            out_specs=vm,
            scratch_shapes=[
                v((tokens, width), BF16),
                v((tokens, width), BF16),
                v((tokens, width), BF16),
                v((tokens, full), BF16),
                v((7, full, width), BF16),
                v((width, full), BF16),
                v((width, full), BF16),
                v((tokens, width), F32),
                v((3, tc, width), BF16),
                v((4, tokens, width), BF16),
                v((tokens + 8, width), F32),
                v((heads, DV, DK), F32),
                v((1, width), F32),
                v((BLK, 2 * BLK), BF16),
                v((1, full), F32),
                v((3, tokens, width), F32),
                v((tokens, DK), F32),
                v((tokens, width), F32),
                v((tokens, width), BF16),
                v((n_sp, mrows, DK), F32),
                v((n_sp, mrows, DK), BF16),
                v((n_sp, mrows, DK), BF16),
                v((n_sp, rows, DK), F32),
                v((n_sp, rows, DK), BF16),
                v((n_sp, rows, DK), BF16),
                v((8, width), F32),
                v((8, width), F32),
                v((heads, DK, DV), F32),
                v((tokens, width), BF16),
                v((tokens, width), BF16),
                v((tokens, full), F32),
                v((2, tb, cols), BF16),
                v((2, 2, tb, cols), BF16),
                v((tb, cols), BF16),
                v((tb, cols), BF16),
                v((2, tb, cols), BF16),
                v((2, tb, cols), BF16),
                v((2, tb, cols), F32),
                pltpu.SemaphoreType.REGULAR((4,)),
                dma((7, 4)),
                dma((3,)),
            ]
            + [dma((2 * chunks,))] * 8
            + [dma((n_sp,))] * 4
            + [dma] * 6
            + [dma((2,))] * 4,
            compiler_params=pltpu.CompilerParams(
                collective_id=0, has_side_effects=True, vmem_limit_bytes=VMEM_LIMIT
            ),
            name="layer",
        )(x, ing, surge, fmin.reshape(1, width), taps, hgain.reshape(1, DV), start, ong,
          wq, wf, wval, wpre, wcv, wpost, wog, wr, wc)

    in_specs = (
        P("sp", "tp"),
        P(),
        P(None, "tp"),
        P(None, "tp"),
        P(None, "tp"),
        P(None, "tp"),
        P(None, "tp"),
        P(None, "tp"),
        P(None, "tp"),
        P("tp"),
        P("sp", "tp"),
        P(None, "tp"),
        P(),
        P("tp", "sp", None),
        P("tp", None),
        P("tp", None),
        P(),
    )
    return jax.shard_map(
        body, mesh=mesh, in_specs=in_specs, out_specs=P(("sp", "tp"), None), check_vma=False
    )
```

```python
import jax
import jax.numpy as jnp
from jax import lax
from jax.experimental import pallas as pl
from jax.experimental.pallas import tpu as pltpu
from jax.sharding import PartitionSpec as P

DK = 128
DV = 128
BLK = 64
EPS = 1e-06
MESH = pl.DeviceIdType.MESH
F32 = jnp.float32
BF16 = jnp.bfloat16
VMEM_LIMIT = 62 * 1024 * 1024

NT = (((1,), (1,)), ((), ()))
TN = (((0,), (0,)), ((), ()))


def dot(a, b, dims=None):
    if dims is None:
        return jnp.dot(a, b, preferred_element_type=F32)
    return lax.dot_general(a, b, dims, preferred_element_type=F32)


def sigmoid(v):
    return lax.logistic(v)


def log_one_minus(u):
    return -u * (1.0 + u * (1 / 2 + u * (1 / 3 + u * (1 / 4 + u * (1 / 5 + u * (1 / 6))))))


def layer(chunks, n_sp, *refs):
    x, gain, surge, fmin, taps, hgain, start, ogain = refs[:8]
    ws = refs[8:15]
    wr_in, wc_in, out = refs[15:18]
    (xl, xr, xo, xn, wv, wr, wc, sv, pr, pd, mx, state, run, tri2, gains) = refs[18:33]
    (kts, runs, snap, part3, scales, part, qs, stf, st, got, dcol, back, sin, rim, rim_in, sb, rec, cvo, accc) = refs[33:52]
    (po, pp, ra, rb, fl, fr, acc) = refs[52:59]
    known, wsem, msem, s_or, s_ol, s_fr, s_fl, r_l, r_r, r_oa, r_ob = refs[59:70]
    s1, r1, s2, r2, rs, rr = refs[70:76]
    s_a, s_b, r_a, r_b, s_r, s_l, r_fl, r_fr = refs[76:]
    tokens, width = x.shape
    full = 4 * width
    tc = tokens // chunks
    parts = 2 * chunks
    tm = tokens // parts
    half = tm // 2
    heads = width // DK
    own_rows = DK // n_sp
    srows = heads * own_rows
    tb = tokens // 4
    cols = full // 2
    me = lax.axis_index("tp")
    sp = lax.axis_index("sp")
    right, left, opp = lax.rem(me + 1, 4), lax.rem(me + 3, 4), lax.rem(me + 2, 4)
    srcs = (me, left, right, opp)

    first, early, later = [], [], []
    for k in range(7):
        for r in range(4):
            rows = pl.ds(pl.multiple_of(srcs[r] * width, width), width)
            copy = pltpu.make_async_copy(
                ws[k].at[rows, :], wv.at[k, pl.ds(r * width, width), :], wsem.at[k, r]
            )
            (early if r == 0 else first if k < 3 else later).append(copy)
    first.append(pltpu.make_async_copy(surge, sv, msem.at[0]))
    later.append(pltpu.make_async_copy(wr_in, wr, msem.at[1]))
    later.append(pltpu.make_async_copy(wc_in, wc, msem.at[2]))
    for copy in early + first + later:
        copy.start()

    barrier = pltpu.get_barrier_semaphore()
    for peer in (left, right):
        pl.semaphore_signal(barrier, inc=1, device_id={"tp": peer}, device_id_type=MESH)

    def each(f):
        def step(d, carry):
            f(d)
            return carry

        lax.fori_loop(1, n_sp, step, 0)

    def tell(sem, d):
        for to in (lax.rem(sp + d, n_sp), lax.rem(sp + n_sp - d, n_sp)):
            pl.semaphore_signal(sem, inc=1, device_id={"sp": to}, device_id_type=MESH)

    tell(barrier, 1)
    pl.semaphore_wait(barrier, 4)
    rounds = n_sp.bit_length() - 2
    tell(known.at[0], 1)

    def beside(src, dst, ss, rs, to_right):
        return pltpu.make_async_remote_copy(
            src_ref=src,
            dst_ref=dst,
            send_sem=ss,
            recv_sem=rs,
            device_id={"tp": right if to_right else left},
            device_id_type=MESH,
        )

    def along(src, dst, ss, rs, to):
        return pltpu.make_async_remote_copy(
            src_ref=src,
            dst_ref=dst,
            send_sem=ss,
            recv_sem=rs,
            device_id={"sp": to},
            device_id_type=MESH,
        )

    def rows_of(c, size, off=0):
        return pl.ds(pl.multiple_of(c * tc + off, 16), size)

    def own(c, to_right):
        rows = pl.ds(pl.multiple_of(c * tm, 16), tm)
        return beside(
            x.at[rows, :],
            (xl if to_right else xr).at[rows, :],
            (s_or if to_right else s_ol).at[c],
            (r_l if to_right else r_r).at[c],
            to_right,
        )

    def forward(c, to_right):
        rows = pl.ds(pl.multiple_of(c * tm + (0 if to_right else half), 16), half)
        return beside(
            (xl if to_right else xr).at[rows, :],
            xo.at[rows, :],
            (s_fr if to_right else s_fl).at[c],
            (r_oa if to_right else r_ob).at[c],
            to_right,
        )

    def pass_on(c):
        own(c, True).wait_recv()
        forward(c, True).start()
        own(c, False).wait_recv()
        forward(c, False).start()

    def send(c):
        own(c, True).start()
        own(c, False).start()

    send(0)
    send(1)

    state[...] = jnp.zeros_like(state)
    run[...] = jnp.zeros_like(run)
    gains[...] = gain[...].astype(F32).reshape(1, full)
    row = lax.broadcasted_iota(jnp.int32, (BLK, 2 * BLK), 0)
    col = lax.broadcasted_iota(jnp.int32, (BLK, 2 * BLK), 1)
    tri2[...] = jnp.where(row >= lax.rem(col, BLK), 1.0, 0.0).astype(BF16)

    xn[:, 0:width] = (x[...].astype(F32) * gains[:, pl.ds(pl.multiple_of(me * width, width), width)]).astype(BF16)
    for copy in early:
        copy.wait()

    def own_wide(k, carry):
        cs = pl.ds(pl.multiple_of(k * width, width), width)
        accc[:, cs] = dot(xn[:, 0:width], wv[k + 3, 0:width, :])
        return carry

    def own_narrow(k, carry):
        part3[k] = dot(xn[:, 0:width], wv[k, 0:width, :])
        return carry

    lax.fori_loop(0, 3, own_narrow, 0)
    pass_on(0)
    send(2)
    lax.fori_loop(0, 4, own_wide, 0)
    pass_on(1)
    send(3)
    for copy in first:
        copy.wait()

    def outputs(c, carry):
        rows = rows_of(c, tc)
        total = dot(xn[rows, width:], wv[0, width:, :]) + part3[0, rows, :]
        pr[0, rows, :] = (total * scales[rows, 0:1]).astype(BF16)
        for b in range(tc // BLK):
            gr = rows_of(c, BLK, b * BLK)
            block = c * (tc // BLK) + b
            for h in range(heads):
                ln = slice(h * DK, (h + 1) * DK)
                cum = mx[gr, ln]
                ref = cum[BLK // 2 - 1 : BLK // 2, :]
                qraw = pr[0, gr, ln].astype(F32)
                qt = qraw * sigmoid(qraw) * (DK**-0.5) * jnp.exp(cum - ref)
                qc = (qt * jnp.exp(ref)).astype(BF16)
                qs[gr, ln] = (qt * jnp.exp(ref + runs[block, :, ln])).astype(BF16)
                sc = dot(qt.astype(BF16), kts[gr, ln], NT)
                ri = lax.broadcasted_iota(jnp.int32, (BLK, BLK), 0)
                ci = lax.broadcasted_iota(jnp.int32, (BLK, BLK), 1)
                sc = jnp.where(ri >= ci, sc, 0.0).astype(BF16)
                part[gr, ln] = dot(sc, pr[2, gr, ln]) + dot(qc, snap[block, h], NT)
        return carry

    def chunk(c, carry):
        def relay(m):
            @pl.when(m < parts)
            def _():
                pass_on(m)

            @pl.when(m + 2 < parts)
            def _():
                send(m + 2)

        relay(2 * c + 2)
        for m in range(2):
            forward(2 * c + m, True).wait_recv()
            forward(2 * c + m, False).wait_recv()

        rows = rows_of(c, tc)
        total = jnp.zeros((tc, 1), F32)
        for piece in (x, xl, xr, xo):
            v = piece[rows, :].astype(F32)
            total = total + jnp.sum(v * v, axis=1, keepdims=True)
        scale = lax.rsqrt(total * (1.0 / full) + EPS)
        scales[rows, :] = jnp.broadcast_to(scale, (tc, DK))
        for r, piece in ((1, xl), (2, xr), (3, xo)):
            g = gains[:, pl.ds(pl.multiple_of(srcs[r] * width, width), width)]
            xn[rows, r * width : (r + 1) * width] = (piece[rows, :].astype(F32) * g).astype(BF16)

        def project(k, carry):
            total = dot(xn[rows, width:], wv[k, width:, :]) + part3[k, rows, :]
            pr[k, rows, :] = (total * scales[rows, 0:1]).astype(BF16)
            return carry

        lax.fori_loop(1, 3, project, 0)
        relay(2 * c + 3)

        for b in range(tc // BLK):
            gr = rows_of(c, BLK, b * BLK)
            block = c * (tc // BLK) + b
            runs[block] = run[...]
            hl = [slice(h * DK, (h + 1) * DK) for h in range(heads)]
            us = [(1.0 - fmin[:, ln]) * sigmoid(-pr[1, gr, ln].astype(F32)) for ln in hl]
            lgs = [log_one_minus(u) + sv[gr, ln] for u, ln in zip(us, hl)]
            his = [lg.astype(BF16) for lg in lgs]
            los = [(lg - hi.astype(F32)).astype(BF16) for lg, hi in zip(lgs, his)]
            cums = [dot(tri2[...], jnp.concatenate([a, b], axis=0)) for a, b in zip(his, los)]
            for h in range(heads):
                ln, cum = hl[h], cums[h]
                mx[gr, ln] = cum
                ref = cum[BLK // 2 - 1 : BLK // 2, :]
                tot = cum[BLK - 1 : BLK, :]
                kt = us[h] * jnp.exp(ref - cum)
                kts[gr, ln] = kt.astype(BF16)
                kh = (kt * jnp.exp(tot - ref)).astype(BF16)
                sh = state[h]
                snap[block, h] = sh.astype(BF16)
                state[h] = jnp.exp(tot) * sh + dot(pr[2, gr, ln], kh, TN)
                run[:, ln] = run[:, ln] + tot

        @pl.when(c < chunks - 2)
        def _():
            outputs(c, 0)

        for k in range(rounds):

            @pl.when(c == k)
            def _():
                pl.semaphore_wait(known.at[k], 2)
                if k + 1 < rounds:
                    tell(known.at[k + 1], 2 ** (k + 1))

        return carry

    lax.fori_loop(0, chunks, chunk, 0)

    for h in range(heads):
        sh = state[h].T
        decay = jnp.exp(run[:, h * DK : (h + 1) * DK])
        top = decay.astype(BF16).astype(F32)
        for j in range(n_sp):
            stf[j, h * own_rows : (h + 1) * own_rows, :] = sh[j * own_rows : (j + 1) * own_rows]
            stf[j, srows + h : srows + h + 1, :] = top
            stf[j, srows + heads + h : srows + heads + h + 1, :] = decay - top
    for j in range(n_sp):
        st[j] = stf[j].astype(BF16)

    def there(d):
        to = lax.rem(sp + d, n_sp)
        return along(st.at[to], got.at[sp], s1.at[d], r1.at[d], to)

    def again(d):
        to = lax.rem(sp + d, n_sp)
        return along(back.at[to], sin.at[sp], s2.at[d], r2.at[d], to)

    def rim_copy():
        return along(rim, rim_in, rs, rr, lax.rem(sp + 1, n_sp))

    each(lambda d: there(d).start())
    got[sp] = st[sp]

    for copy in later:
        copy.wait()

    def wide(k, carry):
        cs = pl.ds(pl.multiple_of(k * width, width), width)
        total = dot(xn[:, width:], wv[k + 3, width:, :]) + accc[:, cs]
        pd[k] = (total * scales[:, 0:1]).astype(BF16)
        return carry

    lax.fori_loop(chunks - 2, chunks, outputs, 0)
    lax.fori_loop(0, 2, wide, 0)
    mx[0:8, :] = jnp.zeros((8, width), F32)
    piece = tokens // 8

    def mixing(i, carry):
        rows = pl.ds(pl.multiple_of(i * piece, 16), piece)
        mx[pl.ds(pl.multiple_of(i * piece + 8, 8), piece), :] = pd[0, rows, :].astype(F32) * pd[
            1, rows, :
        ].astype(F32)
        return carry

    lax.fori_loop(0, 8, mixing, 0)
    rim[...] = mx[tokens : tokens + 8, :]
    rim_copy().start()

    each(lambda d: there(d).wait_recv())
    hrow = lax.broadcasted_iota(jnp.int32, (srows, DK), 0)
    lane = lax.broadcasted_iota(jnp.int32, (srows, DK), 1)
    pick = lane == sp * own_rows + lax.rem(hrow, own_rows)
    for j in range(n_sp):
        gj = got[j].astype(F32)
        both = gj[srows : srows + heads] + gj[srows + heads : srows + 2 * heads]
        dec = jnp.concatenate(
            [jnp.broadcast_to(both[h : h + 1, :], (own_rows, DK)) for h in range(heads)],
            axis=0,
        )
        one = jnp.sum(jnp.where(pick, dec, 0.0), axis=1, keepdims=True)
        dcol[j] = jnp.broadcast_to(one, (srows, DK))
    cur = jnp.concatenate([start[h] for h in range(heads)], axis=0)
    for j in range(n_sp):
        back[j] = cur.astype(BF16)
        cur = dcol[j] * cur + got[j].astype(F32)[0:srows]

    each(lambda d: again(d).start())
    sin[sp] = back[sp]

    lax.fori_loop(2, 4, wide, 0)
    rim_copy().wait_recv()
    inside = jnp.where(sp == 0, 0.0, 1.0)
    mx[0:8, :] = rim_in[...] * inside
    t = taps[...].astype(F32)

    def convolve(i, carry):
        rows = pl.ds(pl.multiple_of(i * piece, 16), piece)
        v = mx[pl.ds(pl.multiple_of(i * piece, 8), piece + 8), :]
        conv = v[6 : 6 + piece] * t[0:1] + v[7 : 7 + piece] * t[1:2] + v[8:] * t[2:3]
        cvo[rows, :] = (pd[2, rows, :].astype(F32) * conv).astype(BF16)
        return carry

    lax.fori_loop(0, 8, convolve, 0)

    step = 512 if cols % 512 == 0 else cols

    def conv_part(n, carry):
        cs = pl.ds(pl.multiple_of(n * step, step), step)
        accc[:, cs] = dot(cvo[...], wc[:, cs])
        return carry

    lax.fori_loop(0, full // step, conv_part, 0)

    each(lambda d: again(d).wait_recv())
    for i in range(n_sp):
        si = sin[i].astype(F32)
        for h in range(heads):
            sb[h, i * own_rows : (i + 1) * own_rows, :] = si[h * own_rows : (h + 1) * own_rows, :]

    hg = hgain[...].astype(F32)

    def block_rows(owner):
        return pl.ds(pl.multiple_of(owner * tb, 16), tb)

    def mix_heads(owner):
        rows = block_rows(owner)
        for h in range(heads):
            ln = slice(h * DK, (h + 1) * DK)
            o = part[rows, ln] + dot(qs[rows, ln], sb[h].astype(BF16))
            o = o * lax.rsqrt(jnp.mean(o * o, axis=-1, keepdims=True) + EPS) * hg
            g = pd[3, rows, ln].astype(F32)
            rec[rows, ln] = (o * (g * sigmoid(g))).astype(BF16)

    def product(owner, side, put):
        rows = block_rows(owner)

        def one(n, carry):
            cs = pl.ds(pl.multiple_of(n * step, step), step)
            ns = pl.ds(pl.multiple_of(side * cols + n * step, step), step)
            put(cs, dot(rec[rows, :], wr[:, ns]) + accc[rows, ns])
            return carry

        lax.fori_loop(0, cols // step, one, 0)

    far_a = beside(po.at[0], ra, s_a, r_a, True)
    far_b = beside(po.at[1], rb, s_b, r_b, False)
    near_r = [beside(pp.at[0, s], fl.at[s], s_r.at[s], r_fl.at[s], True) for s in range(2)]
    near_l = [beside(pp.at[1, s], fr.at[s], s_l.at[s], r_fr.at[s], False) for s in range(2)]

    def store(ref):
        def put(cs, v):
            ref[:, cs] = v.astype(BF16)

        return put

    def store_sum(ref, other):
        def put(cs, v):
            ref[:, cs] = (v + other[:, cs].astype(F32)).astype(BF16)

        return put

    def keep(side):
        def put(cs, v):
            acc[side, :, cs] = v

        return put

    mix_heads(opp)
    product(opp, 0, store(po.at[0]))
    far_a.start()
    product(opp, 1, store(po.at[1]))
    far_b.start()
    mix_heads(right)
    product(right, 1, store(pp.at[0, 1]))
    near_r[1].start()
    mix_heads(left)
    product(left, 0, store(pp.at[1, 0]))
    near_l[0].start()
    mix_heads(me)
    for side in range(2):
        product(me, side, keep(side))
    far_a.wait_recv()
    product(right, 0, store_sum(pp.at[0, 0], ra))
    near_r[0].start()
    far_b.wait_recv()
    product(left, 1, store_sum(pp.at[1, 1], rb))
    near_l[1].start()

    sq = jnp.zeros((tb, 1), F32)
    for side in (1, 0):
        near_r[side].wait_recv()
        near_l[side].wait_recv()
        for n in range(cols // step):
            cs = slice(n * step, (n + 1) * step)
            v = acc[side, :, cs] + fl[side, :, cs].astype(F32) + fr[side, :, cs].astype(F32)
            acc[side, :, cs] = v
            sq = sq + jnp.sum(v * v, axis=1, keepdims=True)
    scale = lax.rsqrt(sq * (1.0 / full) + EPS)
    gains[...] = ogain[...].astype(F32).reshape(1, full)
    for side in range(2):
        for n in range(cols // step):
            cs = slice(n * step, (n + 1) * step)
            gs = slice(side * cols + n * step, side * cols + (n + 1) * step)
            out[:, gs] = (acc[side, :, cs] * scale * gains[:, gs]).astype(BF16)

    def finish(c, carry):
        own(c, True).wait_send()
        own(c, False).wait_send()
        forward(c, True).wait_send()
        forward(c, False).wait_send()
        return carry

    lax.fori_loop(0, parts, finish, 0)

    def drain(d):
        there(d).wait_send()
        again(d).wait_send()

    each(drain)
    rim_copy().wait_send()
    far_a.wait_send()
    far_b.wait_send()
    for s in range(2):
        near_r[s].wait_send()
        near_l[s].wait_send()


def solution(mesh):
    n_sp = mesh.shape["sp"]
    vm = pl.BlockSpec(memory_space=pltpu.VMEM)
    hbm = pl.BlockSpec(memory_space=pl.ANY)
    dma = pltpu.SemaphoreType.DMA
    chunks = 4

    def body(x, ing, wq, wf, wval, wog, wpost, wpre, wcv, fmin, surge, taps, hgain, start, wr, wc, ong):
        tokens, width = x.shape
        heads = width // DK
        own_rows = DK // n_sp
        rows = heads * own_rows
        mrows = rows + 2 * heads
        tb = tokens // 4
        full = 4 * width
        cols = full // 2
        v = pltpu.VMEM
        return pl.pallas_call(
            lambda *refs: layer(chunks, n_sp, *refs),
            out_shape=jax.ShapeDtypeStruct((tb, full), BF16),
            in_specs=[vm, vm, hbm, vm, vm, vm, vm, vm] + [hbm] * 9,
            out_specs=vm,
            scratch_shapes=[
                v((tokens, width), BF16),
                v((tokens, width), BF16),
                v((tokens, width), BF16),
                v((tokens, full), BF16),
                v((7, full, width), BF16),
                v((width, full), BF16),
                v((width, full), BF16),
                v((tokens, width), F32),
                v((3, tokens, width), BF16),
                v((4, tokens, width), BF16),
                v((tokens + 8, width), F32),
                v((heads, DV, DK), F32),
                v((1, width), F32),
                v((BLK, 2 * BLK), BF16),
                v((1, full), F32),
                v((tokens, width), BF16),
                v((tokens // BLK, 1, width), F32),
                v((tokens // BLK, heads, DV, DK), BF16),
                v((3, tokens, width), F32),
                v((tokens, DK), F32),
                v((tokens, width), F32),
                v((tokens, width), BF16),
                v((n_sp, mrows, DK), F32),
                v((n_sp, mrows, DK), BF16),
                v((n_sp, mrows, DK), BF16),
                v((n_sp, rows, DK), F32),
                v((n_sp, rows, DK), BF16),
                v((n_sp, rows, DK), BF16),
                v((8, width), F32),
                v((8, width), F32),
                v((heads, DK, DV), F32),
                v((tokens, width), BF16),
                v((tokens, width), BF16),
                v((tokens, full), F32),
                v((2, tb, cols), BF16),
                v((2, 2, tb, cols), BF16),
                v((tb, cols), BF16),
                v((tb, cols), BF16),
                v((2, tb, cols), BF16),
                v((2, tb, cols), BF16),
                v((2, tb, cols), F32),
                pltpu.SemaphoreType.REGULAR((4,)),
                dma((7, 4)),
                dma((3,)),
            ]
            + [dma((2 * chunks,))] * 8
            + [dma((n_sp,))] * 4
            + [dma] * 6
            + [dma((2,))] * 4,
            compiler_params=pltpu.CompilerParams(
                collective_id=0, has_side_effects=True, vmem_limit_bytes=VMEM_LIMIT
            ),
            name="layer",
        )(x, ing, surge, fmin.reshape(1, width), taps, hgain.reshape(1, DV), start, ong,
          wq, wf, wval, wpre, wcv, wpost, wog, wr, wc)

    in_specs = (
        P("sp", "tp"),
        P(),
        P(None, "tp"),
        P(None, "tp"),
        P(None, "tp"),
        P(None, "tp"),
        P(None, "tp"),
        P(None, "tp"),
        P(None, "tp"),
        P("tp"),
        P("sp", "tp"),
        P(None, "tp"),
        P(),
        P("tp", "sp", None),
        P("tp", None),
        P("tp", None),
        P(),
    )
    return jax.shard_map(
        body, mesh=mesh, in_specs=in_specs, out_specs=P(("sp", "tp"), None), check_vma=False
    )
```

```python
import jax
import jax.numpy as jnp
from jax import lax
from jax.experimental import pallas as pl
from jax.experimental.pallas import tpu as pltpu
from jax.sharding import PartitionSpec as P

DK = 128
DV = 128
BLK = 64
EPS = 1e-06
MESH = pl.DeviceIdType.MESH
F32 = jnp.float32
BF16 = jnp.bfloat16
VMEM_LIMIT = 62 * 1024 * 1024

NT = (((1,), (1,)), ((), ()))
TN = (((0,), (0,)), ((), ()))


def dot(a, b, dims=None):
    if dims is None:
        return jnp.dot(a, b, preferred_element_type=F32)
    return lax.dot_general(a, b, dims, preferred_element_type=F32)


def sigmoid(v):
    return lax.logistic(v)


def log_one_minus(u):
    return -u * (1.0 + u * (1 / 2 + u * (1 / 3 + u * (1 / 4 + u * (1 / 5 + u * (1 / 6))))))


def layer(chunks, n_sp, *refs):
    x, gain, surge, fmin, taps, hgain, start, ogain = refs[:8]
    ws = refs[8:15]
    wr_in, wc_in, out = refs[15:18]
    (xl, xr, xo, xn, wv, wr, wc, sv, pr, pd, mx, state, run, tri2, gains) = refs[18:33]
    (kts, runs, snap, part3, scales, part, qs, stf, st, got, dcol, back, sin, rim, rim_in, sb, rec, cvo, accc) = refs[33:52]
    (po, pp, ra, fl, fr, acc) = refs[52:58]
    known, wsem, msem, s_or, s_ol, s_fr, s_fl, r_l, r_r, r_oa, r_ob = refs[58:69]
    s1, r1, s2, r2, rs, rr = refs[69:75]
    s_a, r_a, s_r, s_l, r_fl, r_fr = refs[75:]
    tokens, width = x.shape
    full = 4 * width
    tc = tokens // chunks
    parts = 2 * chunks
    tm = tokens // parts
    half = tm // 2
    heads = width // DK
    own_rows = DK // n_sp
    srows = heads * own_rows
    tb = tokens // 4
    me = lax.axis_index("tp")
    sp = lax.axis_index("sp")
    right, left, opp = lax.rem(me + 1, 4), lax.rem(me + 3, 4), lax.rem(me + 2, 4)
    srcs = (me, left, right, opp)

    first, early, later = [], [], []
    for k in range(7):
        for r in range(4):
            rows = pl.ds(pl.multiple_of(srcs[r] * width, width), width)
            copy = pltpu.make_async_copy(
                ws[k].at[rows, :], wv.at[k, pl.ds(r * width, width), :], wsem.at[k, r]
            )
            (early if r == 0 else first if k < 3 else later).append(copy)
    first.append(pltpu.make_async_copy(surge, sv, msem.at[0]))
    later.append(pltpu.make_async_copy(wr_in, wr, msem.at[1]))
    later.append(pltpu.make_async_copy(wc_in, wc, msem.at[2]))
    for copy in early + first + later:
        copy.start()

    barrier = pltpu.get_barrier_semaphore()
    for peer in (left, right):
        pl.semaphore_signal(barrier, inc=1, device_id={"tp": peer}, device_id_type=MESH)

    def each(f):
        def step(d, carry):
            f(d)
            return carry

        lax.fori_loop(1, n_sp, step, 0)

    def tell(sem, d):
        for to in (lax.rem(sp + d, n_sp), lax.rem(sp + n_sp - d, n_sp)):
            pl.semaphore_signal(sem, inc=1, device_id={"sp": to}, device_id_type=MESH)

    tell(barrier, 1)
    pl.semaphore_wait(barrier, 4)
    rounds = n_sp.bit_length() - 2
    tell(known.at[0], 1)

    def beside(src, dst, ss, rs, to_right):
        return pltpu.make_async_remote_copy(
            src_ref=src,
            dst_ref=dst,
            send_sem=ss,
            recv_sem=rs,
            device_id={"tp": right if to_right else left},
            device_id_type=MESH,
        )

    def along(src, dst, ss, rs, to):
        return pltpu.make_async_remote_copy(
            src_ref=src,
            dst_ref=dst,
            send_sem=ss,
            recv_sem=rs,
            device_id={"sp": to},
            device_id_type=MESH,
        )

    def rows_of(c, size, off=0):
        return pl.ds(pl.multiple_of(c * tc + off, 16), size)

    def own(c, to_right):
        rows = pl.ds(pl.multiple_of(c * tm, 16), tm)
        return beside(
            x.at[rows, :],
            (xl if to_right else xr).at[rows, :],
            (s_or if to_right else s_ol).at[c],
            (r_l if to_right else r_r).at[c],
            to_right,
        )

    def forward(c, to_right):
        rows = pl.ds(pl.multiple_of(c * tm + (0 if to_right else half), 16), half)
        return beside(
            (xl if to_right else xr).at[rows, :],
            xo.at[rows, :],
            (s_fr if to_right else s_fl).at[c],
            (r_oa if to_right else r_ob).at[c],
            to_right,
        )

    def pass_on(c):
        own(c, True).wait_recv()
        forward(c, True).start()
        own(c, False).wait_recv()
        forward(c, False).start()

    def send(c):
        own(c, True).start()
        own(c, False).start()

    send(0)
    send(1)

    state[...] = jnp.zeros_like(state)
    run[...] = jnp.zeros_like(run)
    gains[...] = gain[...].astype(F32).reshape(1, full)
    row = lax.broadcasted_iota(jnp.int32, (BLK, 2 * BLK), 0)
    col = lax.broadcasted_iota(jnp.int32, (BLK, 2 * BLK), 1)
    tri2[...] = jnp.where(row >= lax.rem(col, BLK), 1.0, 0.0).astype(BF16)

    xn[:, 0:width] = (x[...].astype(F32) * gains[:, pl.ds(pl.multiple_of(me * width, width), width)]).astype(BF16)
    for copy in early:
        copy.wait()

    def own_wide(k, carry):
        cs = pl.ds(pl.multiple_of(k * width, width), width)
        accc[:, cs] = dot(xn[:, 0:width], wv[k + 3, 0:width, :])
        return carry

    def own_narrow(k, carry):
        part3[k] = dot(xn[:, 0:width], wv[k, 0:width, :])
        return carry

    lax.fori_loop(0, 3, own_narrow, 0)
    pass_on(0)
    send(2)
    lax.fori_loop(0, 4, own_wide, 0)
    pass_on(1)
    send(3)
    for copy in first + later:
        copy.wait()

    def outputs(c, carry):
        rows = rows_of(c, tc)
        total = dot(xn[rows, width:], wv[0, width:, :]) + part3[0, rows, :]
        pr[0, rows, :] = (total * scales[rows, 0:1]).astype(BF16)
        for b in range(tc // BLK):
            gr = rows_of(c, BLK, b * BLK)
            block = c * (tc // BLK) + b
            for h in range(heads):
                ln = slice(h * DK, (h + 1) * DK)
                cum = mx[gr, ln]
                ref = cum[BLK // 2 - 1 : BLK // 2, :]
                qraw = pr[0, gr, ln].astype(F32)
                qt = qraw * sigmoid(qraw) * (DK**-0.5) * jnp.exp(cum - ref)
                qc = (qt * jnp.exp(ref)).astype(BF16)
                qs[gr, ln] = (qt * jnp.exp(ref + runs[block, :, ln])).astype(BF16)
                sc = dot(qt.astype(BF16), kts[gr, ln], NT)
                ri = lax.broadcasted_iota(jnp.int32, (BLK, BLK), 0)
                ci = lax.broadcasted_iota(jnp.int32, (BLK, BLK), 1)
                sc = jnp.where(ri >= ci, sc, 0.0).astype(BF16)
                part[gr, ln] = dot(sc, pr[2, gr, ln]) + dot(qc, snap[block, h], NT)
        return carry

    def wide(k, rows):
        cs = pl.ds(pl.multiple_of(k * width, width), width)
        total = dot(xn[rows, width:], wv[k + 3, width:, :]) + accc[rows, cs]
        pd[k, rows, :] = (total * scales[rows, 0:1]).astype(BF16)

    def wide_chunk(k, c):
        wide(k, rows_of(c, tc))
        return c

    def wide_rest(k, carry):
        wide(k, pl.ds(2 * tc, tokens - 2 * tc))
        return carry

    def chunk(c, carry):
        def relay(m):
            @pl.when(m < parts)
            def _():
                pass_on(m)

            @pl.when(m + 2 < parts)
            def _():
                send(m + 2)

        relay(2 * c + 2)
        for m in range(2):
            forward(2 * c + m, True).wait_recv()
            forward(2 * c + m, False).wait_recv()

        rows = rows_of(c, tc)
        total = jnp.zeros((tc, 1), F32)
        for piece in (x, xl, xr, xo):
            v = piece[rows, :].astype(F32)
            total = total + jnp.sum(v * v, axis=1, keepdims=True)
        scale = lax.rsqrt(total * (1.0 / full) + EPS)
        scales[rows, :] = jnp.broadcast_to(scale, (tc, DK))
        for r, piece in ((1, xl), (2, xr), (3, xo)):
            g = gains[:, pl.ds(pl.multiple_of(srcs[r] * width, width), width)]
            xn[rows, r * width : (r + 1) * width] = (piece[rows, :].astype(F32) * g).astype(BF16)

        def project(k, carry):
            total = dot(xn[rows, width:], wv[k, width:, :]) + part3[k, rows, :]
            pr[k, rows, :] = (total * scales[rows, 0:1]).astype(BF16)
            return carry

        lax.fori_loop(1, 3, project, 0)
        relay(2 * c + 3)

        for b in range(tc // BLK):
            gr = rows_of(c, BLK, b * BLK)
            block = c * (tc // BLK) + b
            runs[block] = run[...]
            hl = [slice(h * DK, (h + 1) * DK) for h in range(heads)]
            us = [(1.0 - fmin[:, ln]) * sigmoid(-pr[1, gr, ln].astype(F32)) for ln in hl]
            lgs = [log_one_minus(u) + sv[gr, ln] for u, ln in zip(us, hl)]
            his = [lg.astype(BF16) for lg in lgs]
            los = [(lg - hi.astype(F32)).astype(BF16) for lg, hi in zip(lgs, his)]
            cums = [dot(tri2[...], jnp.concatenate([a, b], axis=0)) for a, b in zip(his, los)]
            for h in range(heads):
                ln, cum = hl[h], cums[h]
                mx[gr, ln] = cum
                ref = cum[BLK // 2 - 1 : BLK // 2, :]
                tot = cum[BLK - 1 : BLK, :]
                kt = us[h] * jnp.exp(ref - cum)
                kts[gr, ln] = kt.astype(BF16)
                kh = (kt * jnp.exp(tot - ref)).astype(BF16)
                sh = state[h]
                snap[block, h] = sh.astype(BF16)
                state[h] = jnp.exp(tot) * sh + dot(pr[2, gr, ln], kh, TN)
                run[:, ln] = run[:, ln] + tot

        @pl.when(c < chunks - 2)
        def _():
            outputs(c, 0)

        @pl.when((c >= 1) & (c <= 2))
        def _():
            lax.fori_loop(0, 4, wide_chunk, c - 1)

        for k in range(rounds):

            @pl.when(c == k)
            def _():
                pl.semaphore_wait(known.at[k], 2)
                if k + 1 < rounds:
                    tell(known.at[k + 1], 2 ** (k + 1))

        return carry

    lax.fori_loop(0, chunks, chunk, 0)

    for h in range(heads):
        sh = state[h].T
        decay = jnp.exp(run[:, h * DK : (h + 1) * DK])
        top = decay.astype(BF16).astype(F32)
        for j in range(n_sp):
            stf[j, h * own_rows : (h + 1) * own_rows, :] = sh[j * own_rows : (j + 1) * own_rows]
            stf[j, srows + h : srows + h + 1, :] = top
            stf[j, srows + heads + h : srows + heads + h + 1, :] = decay - top
    for j in range(n_sp):
        st[j] = stf[j].astype(BF16)

    def there(d):
        to = lax.rem(sp + d, n_sp)
        return along(st.at[to], got.at[sp], s1.at[d], r1.at[d], to)

    def again(d):
        to = lax.rem(sp + d, n_sp)
        return along(back.at[to], sin.at[sp], s2.at[d], r2.at[d], to)

    def rim_copy():
        return along(rim, rim_in, rs, rr, lax.rem(sp + 1, n_sp))

    each(lambda d: there(d).start())
    got[sp] = st[sp]


    lax.fori_loop(chunks - 2, chunks, outputs, 0)
    lax.fori_loop(0, 2, wide_rest, 0)
    mx[0:8, :] = jnp.zeros((8, width), F32)
    piece = tokens // 8

    def mixing(i, carry):
        rows = pl.ds(pl.multiple_of(i * piece, 16), piece)
        mx[pl.ds(pl.multiple_of(i * piece + 8, 8), piece), :] = pd[0, rows, :].astype(F32) * pd[
            1, rows, :
        ].astype(F32)
        return carry

    lax.fori_loop(0, 8, mixing, 0)
    rim[...] = mx[tokens : tokens + 8, :]
    rim_copy().start()

    each(lambda d: there(d).wait_recv())
    hrow = lax.broadcasted_iota(jnp.int32, (srows, DK), 0)
    lane = lax.broadcasted_iota(jnp.int32, (srows, DK), 1)
    pick = lane == sp * own_rows + lax.rem(hrow, own_rows)
    for j in range(n_sp):
        gj = got[j].astype(F32)
        both = gj[srows : srows + heads] + gj[srows + heads : srows + 2 * heads]
        dec = jnp.concatenate(
            [jnp.broadcast_to(both[h : h + 1, :], (own_rows, DK)) for h in range(heads)],
            axis=0,
        )
        one = jnp.sum(jnp.where(pick, dec, 0.0), axis=1, keepdims=True)
        dcol[j] = jnp.broadcast_to(one, (srows, DK))
    cur = jnp.concatenate([start[h] for h in range(heads)], axis=0)
    for j in range(n_sp):
        back[j] = cur.astype(BF16)
        cur = dcol[j] * cur + got[j].astype(F32)[0:srows]

    each(lambda d: again(d).start())
    sin[sp] = back[sp]

    lax.fori_loop(2, 4, wide_rest, 0)
    rim_copy().wait_recv()
    inside = jnp.where(sp == 0, 0.0, 1.0)
    mx[0:8, :] = rim_in[...] * inside
    t = taps[...].astype(F32)

    def convolve(i, carry):
        rows = pl.ds(pl.multiple_of(i * piece, 16), piece)
        v = mx[pl.ds(pl.multiple_of(i * piece, 8), piece + 8), :]
        conv = v[6 : 6 + piece] * t[0:1] + v[7 : 7 + piece] * t[1:2] + v[8:] * t[2:3]
        cvo[rows, :] = (pd[2, rows, :].astype(F32) * conv).astype(BF16)
        return carry

    lax.fori_loop(0, 8, convolve, 0)

    step = 512

    def conv_part(n, carry):
        cs = pl.ds(pl.multiple_of(n * step, step), step)
        accc[:, cs] = dot(cvo[...], wc[:, cs])
        return carry

    lax.fori_loop(0, full // step, conv_part, 0)

    each(lambda d: again(d).wait_recv())
    for i in range(n_sp):
        si = sin[i].astype(F32)
        for h in range(heads):
            sb[h, i * own_rows : (i + 1) * own_rows, :] = si[h * own_rows : (h + 1) * own_rows, :]

    hg = hgain[...].astype(F32)

    def block_rows(owner):
        return pl.ds(pl.multiple_of(owner * tb, 16), tb)

    def mix_heads(owner):
        rows = block_rows(owner)
        for h in range(heads):
            ln = slice(h * DK, (h + 1) * DK)
            o = part[rows, ln] + dot(qs[rows, ln], sb[h].astype(BF16))
            o = o * lax.rsqrt(jnp.mean(o * o, axis=-1, keepdims=True) + EPS) * hg
            g = pd[3, rows, ln].astype(F32)
            rec[rows, ln] = (o * (g * sigmoid(g))).astype(BF16)

    pieces = full // step
    mid = pieces // 2

    def product(owner, n):
        rows = block_rows(owner)
        ns = slice(n * step, (n + 1) * step)
        return dot(rec[rows, :], wr[:, ns]) + accc[rows, ns]

    def far(n):
        to_right = n < mid
        return beside(po.at[n], ra.at[n], s_a.at[n], r_a.at[n], to_right)

    def near(n, to_right):
        k = 0 if to_right else 1
        return beside(
            pp.at[k, n],
            (fl if to_right else fr).at[n],
            (s_r if to_right else s_l).at[n],
            (r_fl if to_right else r_fr).at[n],
            to_right,
        )

    order = [k // 2 if k % 2 == 0 else mid + k // 2 for k in range(pieces)]
    mix_heads(opp)
    for n in order:
        po[n] = product(opp, n).astype(BF16)
        far(n).start()
    mix_heads(right)
    for n in range(mid, pieces):
        pp[0, n] = product(right, n).astype(BF16)
        near(n, True).start()
    mix_heads(left)
    for n in range(mid):
        pp[1, n] = product(left, n).astype(BF16)
        near(n, False).start()
    mix_heads(me)
    for n in range(pieces):
        acc[n] = product(me, n)
    for n in order:
        to_right = n < mid
        owner, k = (right, 0) if to_right else (left, 1)
        value = product(owner, n)
        far(n).wait_recv()
        pp[k, n] = (value + ra[n].astype(F32)).astype(BF16)
        near(n, to_right).start()

    def add_in(n, to_right):
        near(n, to_right).wait_recv()
        acc[n] = acc[n] + (fl if to_right else fr)[n].astype(F32)

    for k in range(mid):
        add_in(mid + k, True)
        add_in(k, False)
    sq = jnp.zeros((tb, 1), F32)
    for n in order:
        add_in(n, n < mid)
        v = acc[n]
        sq = sq + jnp.sum(v * v, axis=1, keepdims=True)
    scale = lax.rsqrt(sq * (1.0 / full) + EPS)
    gains[...] = ogain[...].astype(F32).reshape(1, full)
    for n in range(pieces):
        ns = slice(n * step, (n + 1) * step)
        out[:, ns] = (acc[n] * scale * gains[:, ns]).astype(BF16)

    def finish(c, carry):
        own(c, True).wait_send()
        own(c, False).wait_send()
        forward(c, True).wait_send()
        forward(c, False).wait_send()
        return carry

    lax.fori_loop(0, parts, finish, 0)

    def drain(d):
        there(d).wait_send()
        again(d).wait_send()

    each(drain)
    rim_copy().wait_send()
    for n in range(pieces):
        far(n).wait_send()
        near(n, True).wait_send()
        near(n, False).wait_send()


def solution(mesh):
    n_sp = mesh.shape["sp"]
    vm = pl.BlockSpec(memory_space=pltpu.VMEM)
    hbm = pl.BlockSpec(memory_space=pl.ANY)
    dma = pltpu.SemaphoreType.DMA
    chunks = 4

    def body(x, ing, wq, wf, wval, wog, wpost, wpre, wcv, fmin, surge, taps, hgain, start, wr, wc, ong):
        tokens, width = x.shape
        heads = width // DK
        own_rows = DK // n_sp
        rows = heads * own_rows
        mrows = rows + 2 * heads
        tb = tokens // 4
        full = 4 * width
        v = pltpu.VMEM
        return pl.pallas_call(
            lambda *refs: layer(chunks, n_sp, *refs),
            out_shape=jax.ShapeDtypeStruct((tb, full), BF16),
            in_specs=[vm, vm, hbm, vm, vm, vm, vm, vm] + [hbm] * 9,
            out_specs=vm,
            scratch_shapes=[
                v((tokens, width), BF16),
                v((tokens, width), BF16),
                v((tokens, width), BF16),
                v((tokens, full), BF16),
                v((7, full, width), BF16),
                v((width, full), BF16),
                v((width, full), BF16),
                v((tokens, width), F32),
                v((3, tokens, width), BF16),
                v((4, tokens, width), BF16),
                v((tokens + 8, width), F32),
                v((heads, DV, DK), F32),
                v((1, width), F32),
                v((BLK, 2 * BLK), BF16),
                v((1, full), F32),
                v((tokens, width), BF16),
                v((tokens // BLK, 1, width), F32),
                v((tokens // BLK, heads, DV, DK), BF16),
                v((3, tokens, width), F32),
                v((tokens, DK), F32),
                v((tokens, width), F32),
                v((tokens, width), BF16),
                v((n_sp, mrows, DK), F32),
                v((n_sp, mrows, DK), BF16),
                v((n_sp, mrows, DK), BF16),
                v((n_sp, rows, DK), F32),
                v((n_sp, rows, DK), BF16),
                v((n_sp, rows, DK), BF16),
                v((8, width), F32),
                v((8, width), F32),
                v((heads, DK, DV), F32),
                v((tokens, width), BF16),
                v((tokens, width), BF16),
                v((tokens, full), F32),
                v((4, tb, full // 4), BF16),
                v((2, 4, tb, full // 4), BF16),
                v((4, tb, full // 4), BF16),
                v((4, tb, full // 4), BF16),
                v((4, tb, full // 4), BF16),
                v((4, tb, full // 4), F32),
                pltpu.SemaphoreType.REGULAR((4,)),
                dma((7, 4)),
                dma((3,)),
            ]
            + [dma((2 * chunks,))] * 8
            + [dma((n_sp,))] * 4
            + [dma] * 2
            + [dma((4,))] * 6,
            compiler_params=pltpu.CompilerParams(
                collective_id=0, has_side_effects=True, vmem_limit_bytes=VMEM_LIMIT
            ),
            name="layer",
        )(x, ing, surge, fmin.reshape(1, width), taps, hgain.reshape(1, DV), start, ong,
          wq, wf, wval, wpre, wcv, wpost, wog, wr, wc)

    in_specs = (
        P("sp", "tp"),
        P(),
        P(None, "tp"),
        P(None, "tp"),
        P(None, "tp"),
        P(None, "tp"),
        P(None, "tp"),
        P(None, "tp"),
        P(None, "tp"),
        P("tp"),
        P("sp", "tp"),
        P(None, "tp"),
        P(),
        P("tp", "sp", None),
        P("tp", None),
        P("tp", None),
        P(),
    )
    return jax.shard_map(
        body, mesh=mesh, in_specs=in_specs, out_specs=P(("sp", "tp"), None), check_vma=False
    )
```

```python
import jax
import jax.numpy as jnp
from jax import lax
from jax.experimental import pallas as pl
from jax.experimental.pallas import tpu as pltpu
from jax.sharding import PartitionSpec as P

DK = 128
DV = 128
BLK = 64
EPS = 1e-06
MESH = pl.DeviceIdType.MESH
F32 = jnp.float32
BF16 = jnp.bfloat16
VMEM_LIMIT = 62 * 1024 * 1024

NT = (((1,), (1,)), ((), ()))
TN = (((0,), (0,)), ((), ()))


def dot(a, b, dims=None):
    if dims is None:
        return jnp.dot(a, b, preferred_element_type=F32)
    return lax.dot_general(a, b, dims, preferred_element_type=F32)


def sigmoid(v):
    return lax.logistic(v)


def log_one_minus(u):
    return -u * (1.0 + u * (1 / 2 + u * (1 / 3 + u * (1 / 4 + u * (1 / 5 + u * (1 / 6))))))


def layer(chunks, n_sp, *refs):
    x, gain, surge, fmin, taps, hgain, start, ogain = refs[:8]
    ws = refs[8:15]
    wr_in, wc_in, out = refs[15:18]
    (xl, xr, xo, xn, wv, wr, wc, sv, pr, pd, mx, state, run, tri2, gains) = refs[18:33]
    (kts, runs, snap, part3, scales, part, qs, stf, st, got, dcol, back, sin, rim, rim_in, sb, rec, cvo, accc) = refs[33:52]
    (po, pp, ra, fl, fr, acc) = refs[52:58]
    known, wsem, msem, s_or, s_ol, s_fr, s_fl, r_l, r_r, r_oa, r_ob = refs[58:69]
    s1, r1, s2, r2, rs, rr = refs[69:75]
    s_a, r_a, s_r, s_l, r_fl, r_fr = refs[75:]
    tokens, width = x.shape
    full = 4 * width
    tc = tokens // chunks
    parts = 2 * chunks
    tm = tokens // parts
    half = tm // 2
    heads = width // DK
    own_rows = DK // n_sp
    srows = heads * own_rows
    tb = tokens // 4
    me = lax.axis_index("tp")
    sp = lax.axis_index("sp")
    right, left, opp = lax.rem(me + 1, 4), lax.rem(me + 3, 4), lax.rem(me + 2, 4)
    srcs = (me, left, right, opp)

    first, early, later = [], [], []
    for k in range(7):
        for r in range(4):
            rows = pl.ds(pl.multiple_of(srcs[r] * width, width), width)
            copy = pltpu.make_async_copy(
                ws[k].at[rows, :], wv.at[k, pl.ds(r * width, width), :], wsem.at[k, r]
            )
            (early if r == 0 else first if k < 3 else later).append(copy)
    first.append(pltpu.make_async_copy(surge, sv, msem.at[0]))
    later.append(pltpu.make_async_copy(wr_in, wr, msem.at[1]))
    later.append(pltpu.make_async_copy(wc_in, wc, msem.at[2]))
    for copy in early + first + later:
        copy.start()

    barrier = pltpu.get_barrier_semaphore()
    for peer in (left, right):
        pl.semaphore_signal(barrier, inc=1, device_id={"tp": peer}, device_id_type=MESH)

    def each(f):
        def step(d, carry):
            f(d)
            return carry

        lax.fori_loop(1, n_sp, step, 0)

    def tell(sem, d):
        @pl.when(sp + d < n_sp)
        def _():
            pl.semaphore_signal(sem, inc=1, device_id={"sp": sp + d}, device_id_type=MESH)

        @pl.when(sp >= d)
        def _():
            pl.semaphore_signal(sem, inc=1, device_id={"sp": sp - d}, device_id_type=MESH)

    def beyond(d):
        return jnp.where(sp + d < n_sp, 1, 0) + jnp.where(sp >= d, 1, 0)

    def hear(sem, d):
        pl.semaphore_wait(sem, beyond(d))

    tell(barrier, 1)
    pl.semaphore_wait(barrier, 2 + beyond(1))
    rounds = n_sp.bit_length() - 1
    tell(known.at[0], 1)

    def beside(src, dst, ss, rs, to_right):
        return pltpu.make_async_remote_copy(
            src_ref=src,
            dst_ref=dst,
            send_sem=ss,
            recv_sem=rs,
            device_id={"tp": right if to_right else left},
            device_id_type=MESH,
        )

    def along(src, dst, ss, rs, to):
        return pltpu.make_async_remote_copy(
            src_ref=src,
            dst_ref=dst,
            send_sem=ss,
            recv_sem=rs,
            device_id={"sp": to},
            device_id_type=MESH,
        )

    def rows_of(c, size, off=0):
        return pl.ds(pl.multiple_of(c * tc + off, 16), size)

    def own(c, to_right):
        rows = pl.ds(pl.multiple_of(c * tm, 16), tm)
        return beside(
            x.at[rows, :],
            (xl if to_right else xr).at[rows, :],
            (s_or if to_right else s_ol).at[c],
            (r_l if to_right else r_r).at[c],
            to_right,
        )

    def forward(c, to_right):
        rows = pl.ds(pl.multiple_of(c * tm + (0 if to_right else half), 16), half)
        return beside(
            (xl if to_right else xr).at[rows, :],
            xo.at[rows, :],
            (s_fr if to_right else s_fl).at[c],
            (r_oa if to_right else r_ob).at[c],
            to_right,
        )

    def pass_on(c):
        own(c, True).wait_recv()
        forward(c, True).start()
        own(c, False).wait_recv()
        forward(c, False).start()

    def send(c):
        own(c, True).start()
        own(c, False).start()

    send(0)
    send(1)

    state[...] = jnp.zeros_like(state)
    run[...] = jnp.zeros_like(run)
    gains[...] = gain[...].astype(F32).reshape(1, full)
    row = lax.broadcasted_iota(jnp.int32, (BLK, 2 * BLK), 0)
    col = lax.broadcasted_iota(jnp.int32, (BLK, 2 * BLK), 1)
    tri2[...] = jnp.where(row >= lax.rem(col, BLK), 1.0, 0.0).astype(BF16)

    xn[:, 0:width] = (x[...].astype(F32) * gains[:, pl.ds(pl.multiple_of(me * width, width), width)]).astype(BF16)
    for copy in early:
        copy.wait()

    def own_wide(k, carry):
        cs = pl.ds(pl.multiple_of(k * width, width), width)
        accc[:, cs] = dot(xn[:, 0:width], wv[k + 3, 0:width, :])
        return carry

    def own_narrow(k, carry):
        part3[k] = dot(xn[:, 0:width], wv[k, 0:width, :])
        return carry

    lax.fori_loop(0, 3, own_narrow, 0)
    pass_on(0)
    send(2)
    lax.fori_loop(0, 4, own_wide, 0)
    pass_on(1)
    send(3)
    for copy in first + later:
        copy.wait()

    hear(known.at[0], 1)
    tell(known.at[1], 2)

    def outputs(c, carry):
        rows = rows_of(c, tc)
        total = dot(xn[rows, width:], wv[0, width:, :]) + part3[0, rows, :]
        pr[0, rows, :] = (total * scales[rows, 0:1]).astype(BF16)
        for b in range(tc // BLK):
            gr = rows_of(c, BLK, b * BLK)
            block = c * (tc // BLK) + b
            hl = [slice(h * DK, (h + 1) * DK) for h in range(heads)]
            cums = [mx[gr, ln] for ln in hl]
            refs_h = [cum[BLK // 2 - 1 : BLK // 2, :] for cum in cums]
            raws = [pr[0, gr, ln].astype(F32) for ln in hl]
            qts = [
                qraw * sigmoid(qraw) * (DK**-0.5) * jnp.exp(cum - ref)
                for qraw, cum, ref in zip(raws, cums, refs_h)
            ]
            qcs = [(qt * jnp.exp(ref)).astype(BF16) for qt, ref in zip(qts, refs_h)]
            ri = lax.broadcasted_iota(jnp.int32, (BLK, BLK), 0)
            ci = lax.broadcasted_iota(jnp.int32, (BLK, BLK), 1)
            scs = [dot(qt.astype(BF16), kts[gr, ln], NT) for qt, ln in zip(qts, hl)]
            crs = [dot(qc, snap[block, h], NT) for h, qc in enumerate(qcs)]
            scs = [jnp.where(ri >= ci, sc, 0.0).astype(BF16) for sc in scs]
            outs = [dot(sc, pr[2, gr, ln]) + cr for sc, ln, cr in zip(scs, hl, crs)]
            for h, ln in enumerate(hl):
                qs[gr, ln] = (qts[h] * jnp.exp(refs_h[h] + runs[block, :, ln])).astype(BF16)
                part[gr, ln] = outs[h]
        return carry

    def wide(k, rows):
        cs = pl.ds(pl.multiple_of(k * width, width), width)
        total = dot(xn[rows, width:], wv[k + 3, width:, :]) + accc[rows, cs]
        pd[k, rows, :] = (total * scales[rows, 0:1]).astype(BF16)

    def wide_chunk(k, c):
        wide(k, rows_of(c, tc))
        return c

    def wide_rest(k, carry):
        wide(k, pl.ds(2 * tc, tokens - 2 * tc))
        return carry

    def chunk(c, carry):
        def relay(m):
            @pl.when(m < parts)
            def _():
                pass_on(m)

            @pl.when(m + 2 < parts)
            def _():
                send(m + 2)

        relay(2 * c + 2)
        for m in range(2):
            forward(2 * c + m, True).wait_recv()
            forward(2 * c + m, False).wait_recv()

        rows = rows_of(c, tc)
        total = jnp.zeros((tc, 1), F32)
        for piece in (x, xl, xr, xo):
            v = piece[rows, :].astype(F32)
            total = total + jnp.sum(v * v, axis=1, keepdims=True)
        scale = lax.rsqrt(total * (1.0 / full) + EPS)
        scales[rows, :] = jnp.broadcast_to(scale, (tc, DK))
        for r, piece in ((1, xl), (2, xr), (3, xo)):
            g = gains[:, pl.ds(pl.multiple_of(srcs[r] * width, width), width)]
            xn[rows, r * width : (r + 1) * width] = (piece[rows, :].astype(F32) * g).astype(BF16)

        def project(k, carry):
            total = dot(xn[rows, width:], wv[k, width:, :]) + part3[k, rows, :]
            pr[k, rows, :] = (total * scales[rows, 0:1]).astype(BF16)
            return carry

        lax.fori_loop(1, 3, project, 0)
        relay(2 * c + 3)

        for b in range(tc // BLK):
            gr = rows_of(c, BLK, b * BLK)
            block = c * (tc // BLK) + b
            runs[block] = run[...]
            hl = [slice(h * DK, (h + 1) * DK) for h in range(heads)]
            us = [(1.0 - fmin[:, ln]) * sigmoid(-pr[1, gr, ln].astype(F32)) for ln in hl]
            lgs = [log_one_minus(u) + sv[gr, ln] for u, ln in zip(us, hl)]
            his = [lg.astype(BF16) for lg in lgs]
            los = [(lg - hi.astype(F32)).astype(BF16) for lg, hi in zip(lgs, his)]
            cums = [dot(tri2[...], jnp.concatenate([a, b], axis=0)) for a, b in zip(his, los)]
            for h in range(heads):
                ln, cum = hl[h], cums[h]
                mx[gr, ln] = cum
                ref = cum[BLK // 2 - 1 : BLK // 2, :]
                tot = cum[BLK - 1 : BLK, :]
                kt = us[h] * jnp.exp(ref - cum)
                kts[gr, ln] = kt.astype(BF16)
                kh = (kt * jnp.exp(tot - ref)).astype(BF16)
                sh = state[h]
                snap[block, h] = sh.astype(BF16)
                state[h] = jnp.exp(tot) * sh + dot(pr[2, gr, ln], kh, TN)
                run[:, ln] = run[:, ln] + tot

        @pl.when(c < chunks - 2)
        def _():
            outputs(c, 0)

        @pl.when((c >= 1) & (c <= 2))
        def _():
            lax.fori_loop(0, 4, wide_chunk, c - 1)

        for k in range(1, rounds):

            @pl.when(c == k - 1)
            def _():
                hear(known.at[k], 2**k)
                if k + 1 < rounds:
                    tell(known.at[k + 1], 2 ** (k + 1))

        return carry

    lax.fori_loop(0, chunks, chunk, 0)

    for h in range(heads):
        sh = state[h].T
        decay = jnp.exp(run[:, h * DK : (h + 1) * DK])
        top = decay.astype(BF16).astype(F32)
        for j in range(n_sp):
            stf[j, h * own_rows : (h + 1) * own_rows, :] = sh[j * own_rows : (j + 1) * own_rows]
            stf[j, srows + h : srows + h + 1, :] = top
            stf[j, srows + heads + h : srows + heads + h + 1, :] = decay - top
    for j in range(n_sp):
        st[j] = stf[j].astype(BF16)

    def there(d):
        to = lax.rem(sp + d, n_sp)
        return along(st.at[to], got.at[sp], s1.at[d], r1.at[d], to)

    def again(d):
        to = lax.rem(sp + d, n_sp)
        return along(back.at[to], sin.at[sp], s2.at[d], r2.at[d], to)

    def rim_copy():
        return along(rim, rim_in, rs, rr, lax.rem(sp + 1, n_sp))

    each(lambda d: there(d).start())
    got[sp] = st[sp]


    lax.fori_loop(chunks - 2, chunks, outputs, 0)
    lax.fori_loop(0, 2, wide_rest, 0)
    mx[0:8, :] = jnp.zeros((8, width), F32)
    piece = tokens // 8

    def mixing(i, carry):
        rows = pl.ds(pl.multiple_of(i * piece, 16), piece)
        mx[pl.ds(pl.multiple_of(i * piece + 8, 8), piece), :] = pd[0, rows, :].astype(F32) * pd[
            1, rows, :
        ].astype(F32)
        return carry

    lax.fori_loop(0, 8, mixing, 0)
    rim[...] = mx[tokens : tokens + 8, :]
    rim_copy().start()

    each(lambda d: there(d).wait_recv())
    hrow = lax.broadcasted_iota(jnp.int32, (srows, DK), 0)
    lane = lax.broadcasted_iota(jnp.int32, (srows, DK), 1)
    pick = lane == sp * own_rows + lax.rem(hrow, own_rows)
    for j in range(n_sp):
        gj = got[j].astype(F32)
        both = gj[srows : srows + heads] + gj[srows + heads : srows + 2 * heads]
        dec = jnp.concatenate(
            [jnp.broadcast_to(both[h : h + 1, :], (own_rows, DK)) for h in range(heads)],
            axis=0,
        )
        one = jnp.sum(jnp.where(pick, dec, 0.0), axis=1, keepdims=True)
        dcol[j] = jnp.broadcast_to(one, (srows, DK))
    cur = jnp.concatenate([start[h] for h in range(heads)], axis=0)
    for j in range(n_sp):
        back[j] = cur.astype(BF16)
        cur = dcol[j] * cur + got[j].astype(F32)[0:srows]

    each(lambda d: again(d).start())
    sin[sp] = back[sp]

    lax.fori_loop(2, 4, wide_rest, 0)
    rim_copy().wait_recv()
    inside = jnp.where(sp == 0, 0.0, 1.0)
    mx[0:8, :] = rim_in[...] * inside
    t = taps[...].astype(F32)

    def convolve(i, carry):
        rows = pl.ds(pl.multiple_of(i * piece, 16), piece)
        v = mx[pl.ds(pl.multiple_of(i * piece, 8), piece + 8), :]
        conv = v[6 : 6 + piece] * t[0:1] + v[7 : 7 + piece] * t[1:2] + v[8:] * t[2:3]
        cvo[rows, :] = (pd[2, rows, :].astype(F32) * conv).astype(BF16)
        return carry

    lax.fori_loop(0, 8, convolve, 0)

    step = 512

    def conv_part(n, carry):
        cs = pl.ds(pl.multiple_of(n * step, step), step)
        accc[:, cs] = dot(cvo[...], wc[:, cs])
        return carry

    lax.fori_loop(0, full // step, conv_part, 0)

    each(lambda d: again(d).wait_recv())
    for i in range(n_sp):
        si = sin[i].astype(F32)
        for h in range(heads):
            sb[h, i * own_rows : (i + 1) * own_rows, :] = si[h * own_rows : (h + 1) * own_rows, :]

    hg = hgain[...].astype(F32)

    def block_rows(owner):
        return pl.ds(pl.multiple_of(owner * tb, 16), tb)

    def mix_heads(owner):
        rows = block_rows(owner)
        for h in range(heads):
            ln = slice(h * DK, (h + 1) * DK)
            o = part[rows, ln] + dot(qs[rows, ln], sb[h].astype(BF16))
            o = o * lax.rsqrt(jnp.mean(o * o, axis=-1, keepdims=True) + EPS) * hg
            g = pd[3, rows, ln].astype(F32)
            rec[rows, ln] = (o * (g * sigmoid(g))).astype(BF16)

    pieces = full // step
    mid = pieces // 2

    def product(owner, n):
        rows = block_rows(owner)
        ns = slice(n * step, (n + 1) * step)
        return dot(rec[rows, :], wr[:, ns]) + accc[rows, ns]

    def far(n):
        to_right = n < mid
        return beside(po.at[n], ra.at[n], s_a.at[n], r_a.at[n], to_right)

    def near(n, to_right):
        k = 0 if to_right else 1
        return beside(
            pp.at[k, n],
            (fl if to_right else fr).at[n],
            (s_r if to_right else s_l).at[n],
            (r_fl if to_right else r_fr).at[n],
            to_right,
        )

    order = [k // 2 if k % 2 == 0 else mid + k // 2 for k in range(pieces)]
    mix_heads(opp)
    for n in order:
        po[n] = product(opp, n).astype(BF16)
        far(n).start()
    mix_heads(right)
    for n in range(mid, pieces):
        pp[0, n] = product(right, n).astype(BF16)
        near(n, True).start()
    mix_heads(left)
    for n in range(mid):
        pp[1, n] = product(left, n).astype(BF16)
        near(n, False).start()
    mix_heads(me)
    for n in range(pieces):
        acc[n] = product(me, n)
    for n in order:
        to_right = n < mid
        owner, k = (right, 0) if to_right else (left, 1)
        value = product(owner, n)
        far(n).wait_recv()
        pp[k, n] = (value + ra[n].astype(F32)).astype(BF16)
        near(n, to_right).start()

    def add_in(n, to_right):
        near(n, to_right).wait_recv()
        acc[n] = acc[n] + (fl if to_right else fr)[n].astype(F32)

    for k in range(mid):
        add_in(mid + k, True)
        add_in(k, False)
    sq = jnp.zeros((tb, 1), F32)
    for n in order:
        add_in(n, n < mid)
        v = acc[n]
        sq = sq + jnp.sum(v * v, axis=1, keepdims=True)
    scale = lax.rsqrt(sq * (1.0 / full) + EPS)
    gains[...] = ogain[...].astype(F32).reshape(1, full)
    for n in range(pieces):
        ns = slice(n * step, (n + 1) * step)
        out[:, ns] = (acc[n] * scale * gains[:, ns]).astype(BF16)

    def finish(c, carry):
        own(c, True).wait_send()
        own(c, False).wait_send()
        forward(c, True).wait_send()
        forward(c, False).wait_send()
        return carry

    lax.fori_loop(0, parts, finish, 0)

    def drain(d):
        there(d).wait_send()
        again(d).wait_send()

    each(drain)
    rim_copy().wait_send()
    for n in range(pieces):
        far(n).wait_send()
        near(n, True).wait_send()
        near(n, False).wait_send()


def solution(mesh):
    n_sp = mesh.shape["sp"]
    vm = pl.BlockSpec(memory_space=pltpu.VMEM)
    hbm = pl.BlockSpec(memory_space=pl.ANY)
    dma = pltpu.SemaphoreType.DMA
    chunks = 4

    def body(x, ing, wq, wf, wval, wog, wpost, wpre, wcv, fmin, surge, taps, hgain, start, wr, wc, ong):
        tokens, width = x.shape
        heads = width // DK
        own_rows = DK // n_sp
        rows = heads * own_rows
        mrows = rows + 2 * heads
        tb = tokens // 4
        full = 4 * width
        v = pltpu.VMEM
        return pl.pallas_call(
            lambda *refs: layer(chunks, n_sp, *refs),
            out_shape=jax.ShapeDtypeStruct((tb, full), BF16),
            in_specs=[vm, vm, hbm, vm, vm, vm, vm, vm] + [hbm] * 9,
            out_specs=vm,
            scratch_shapes=[
                v((tokens, width), BF16),
                v((tokens, width), BF16),
                v((tokens, width), BF16),
                v((tokens, full), BF16),
                v((7, full, width), BF16),
                v((width, full), BF16),
                v((width, full), BF16),
                v((tokens, width), F32),
                v((3, tokens, width), BF16),
                v((4, tokens, width), BF16),
                v((tokens + 8, width), F32),
                v((heads, DV, DK), F32),
                v((1, width), F32),
                v((BLK, 2 * BLK), BF16),
                v((1, full), F32),
                v((tokens, width), BF16),
                v((tokens // BLK, 1, width), F32),
                v((tokens // BLK, heads, DV, DK), BF16),
                v((3, tokens, width), F32),
                v((tokens, DK), F32),
                v((tokens, width), F32),
                v((tokens, width), BF16),
                v((n_sp, mrows, DK), F32),
                v((n_sp, mrows, DK), BF16),
                v((n_sp, mrows, DK), BF16),
                v((n_sp, rows, DK), F32),
                v((n_sp, rows, DK), BF16),
                v((n_sp, rows, DK), BF16),
                v((8, width), F32),
                v((8, width), F32),
                v((heads, DK, DV), F32),
                v((tokens, width), BF16),
                v((tokens, width), BF16),
                v((tokens, full), F32),
                v((4, tb, full // 4), BF16),
                v((2, 4, tb, full // 4), BF16),
                v((4, tb, full // 4), BF16),
                v((4, tb, full // 4), BF16),
                v((4, tb, full // 4), BF16),
                v((4, tb, full // 4), F32),
                pltpu.SemaphoreType.REGULAR((5,)),
                dma((7, 4)),
                dma((3,)),
            ]
            + [dma((2 * chunks,))] * 8
            + [dma((n_sp,))] * 4
            + [dma] * 2
            + [dma((4,))] * 6,
            compiler_params=pltpu.CompilerParams(
                collective_id=0, has_side_effects=True, vmem_limit_bytes=VMEM_LIMIT
            ),
            name="layer",
        )(x, ing, surge, fmin.reshape(1, width), taps, hgain.reshape(1, DV), start, ong,
          wq, wf, wval, wpre, wcv, wpost, wog, wr, wc)

    in_specs = (
        P("sp", "tp"),
        P(),
        P(None, "tp"),
        P(None, "tp"),
        P(None, "tp"),
        P(None, "tp"),
        P(None, "tp"),
        P(None, "tp"),
        P(None, "tp"),
        P("tp"),
        P("sp", "tp"),
        P(None, "tp"),
        P(),
        P("tp", "sp", None),
        P("tp", None),
        P("tp", None),
        P(),
    )
    return jax.shard_map(
        body, mesh=mesh, in_specs=in_specs, out_specs=P(("sp", "tp"), None), check_vma=False
    )
```
